256 devices in a mesh: ep: 32 (over z, x), tp: 8 (over y, core).
Axes of the slice: x: 4, y: 4, z: 8, core: 2. Of those that a mesh axis runs over, the one named last changes fastest.
Arguments:
- tokens: bfloat16 [2048, 2048], P('ep'), may hold values from -6 to 6
- norm_gain: float32 [2048], replicated, may hold values from 0.1 to 1.9
- norm_shift: float32 [2048], replicated, may hold values from -3 to 3
- expert_ids: int32 [2048, 4], P('ep'), may hold values from 0 to 63, as said below
- gate_weights: float32 [2048, 4], P('ep'), may hold values from 0.1 to 1
- expert_gate: bfloat16 [64, 2048, 512], P('ep', None, 'tp'), may hold values from -0.125 to 0.125
- expert_up: bfloat16 [64, 2048, 512], P('ep', None, 'tp'), may hold values from -0.125 to 0.125
- expert_down: bfloat16 [64, 512, 2048], P('ep', 'tp'), may hold values from -0.25 to 0.25
Outputs:
- mixed_out: bfloat16 [2048, 2048], P('ep', 'tp')
The draws below stay inside these ranges and needn't reach their ends.
Inputs may be any that keep to these rules, and one draw needn't show every extreme that they name: `expert_ids`: each row names 4 distinct experts that all lie in one group of 16 consecutive expert numbers. In the rows of one index of ep (aligned blocks of 64 rows) no expert is named by more than 8 rows, and in every block some expert is named by exactly 8 rows.
All inputs are finite; a program needn't handle non-finite values.
Results may differ from the reference program's by a relative error of at most 0.002.
Values may be sent and summed in bfloat16 or wider, within the bound.
A program may use at most 64 MiB of HBM per device.

```python
import jax
import jax.numpy as jnp
from jax import lax

D = 2048
F = 512
TOP_K = 4
GROUPS = 4
TOK_DEV = 64
EXPERTS = 64
GROUP_SIZE = 16
CAP = 8
TOKENS = 2048
N_EP = 32


def shuffle_block(block_key):
    return jax.random.permutation(block_key, TOK_DEV)


def draw_expert_ids(key, part):
    key_heavy = jax.random.fold_in(key, 11)
    key_order = jax.random.fold_in(key, 23)
    key_shift = jax.random.fold_in(key, 37)
    heavy = jax.random.randint(key_heavy, (N_EP, 1), 0, GROUPS)
    block_keys = jax.random.split(key_order, N_EP)
    order = jax.vmap(shuffle_block)(block_keys).astype(jnp.int32)
    inverse = jnp.argsort(order, axis=1).astype(jnp.int32)
    half_rows = TOK_DEV // 2
    others = jnp.maximum(inverse - half_rows, 0)
    in_heavy = inverse < half_rows
    group_id = jnp.where(in_heavy, heavy, (heavy + 1 + others % (GROUPS - 1)) % GROUPS)
    ranks = jnp.where(in_heavy, inverse, others // (GROUPS - 1))
    offsets = jax.random.randint(key_shift, (N_EP, GROUPS), 0, GROUP_SIZE)
    shift_rows = jnp.take_along_axis(offsets, group_id, axis=1)
    within = (ranks[:, :, None] * TOP_K + jnp.arange(TOP_K, dtype=jnp.int32)[None, None, :] + shift_rows[:, :, None]) % GROUP_SIZE
    chosen = group_id[:, :, None] * GROUP_SIZE + within
    return chosen.reshape(N_EP * TOK_DEV, TOP_K).astype(jnp.int32)


def levels(key, extent, shards, least, top_value):
    gain = 1.0
    for axis_at, parts in shards:
        steps = jax.random.uniform(jax.random.fold_in(jax.random.fold_in(key, 6), axis_at), (parts,), jnp.float32, least / len(shards), top_value / len(shards))
        gain = gain * jnp.repeat(jnp.exp(steps), extent[axis_at] // parts).reshape((-1,) + (1,) * (len(extent) - 1 - axis_at))
    return gain


def normal_values(own_key, dims, width, limit, shards=(), kind=jnp.bfloat16):
    values = jax.random.normal(own_key, dims, jnp.float32) * width
    if len(shards) > 0:
        values = levels(own_key, dims, shards, -0.22, 0.18) * values
    return jnp.clip(values, min=-limit, max=limit).astype(kind)


def setup_inputs(seed: int = 0) -> dict:
    keys = jax.random.split(jax.random.key(seed), 9)
    tokens = normal_values(keys[0], (TOKENS, D), 1.0, 6.0, ((0, 32),))
    norm_gain = jnp.clip(1.0 + 0.18 * jax.random.normal(keys[1], (D,), jnp.float32), 0.1, 1.9)
    norm_shift = normal_values(keys[2], (D,), 0.5, 3.0, (), jnp.float32)
    expert_ids = draw_expert_ids(jax.random.fold_in(keys[8], 71), 0)
    gate_weights = jnp.clip(0.1 + 0.9 * jax.random.uniform(keys[4], (TOKENS, TOP_K), jnp.float32) ** levels(keys[4], (TOKENS, TOP_K), ((0, 32),), -0.2, 0.2), 0.1, 1.0)
    expert_gate = normal_values(keys[5], (EXPERTS, D, F), D ** -0.5, 0.125, ((0, 32), (2, 8)))
    expert_up = normal_values(keys[6], (EXPERTS, D, F), D ** -0.5, 0.125, ((0, 32), (2, 8)))
    expert_down = normal_values(keys[7], (EXPERTS, F, D), F ** -0.5, 0.25, ((0, 32), (1, 8)))
    return {"tokens": tokens, "norm_gain": norm_gain, "norm_shift": norm_shift, "expert_ids": expert_ids, "gate_weights": gate_weights, "expert_gate": expert_gate, "expert_up": expert_up, "expert_down": expert_down}


epsilon = 1e-05

def layer_norm(tokens, norm_gain, norm_shift):
    values = tokens.astype(jnp.float32)
    centre = lax.optimization_barrier(jnp.mean(values, axis=-1, keepdims=True))
    spread = lax.optimization_barrier(jnp.mean(jnp.square(values - centre), axis=-1, keepdims=True))
    scaled = (values - centre) * lax.rsqrt(spread + epsilon) * norm_gain + norm_shift
    return scaled.astype(jnp.bfloat16)

def reference(tokens, norm_gain, norm_shift, expert_ids, gate_weights, expert_gate, expert_up, expert_down):
    normed = layer_norm(tokens, norm_gain, norm_shift)
    bound_rows = N_EP * CAP

    def one_expert(totals, expert):
        hits = expert_ids == expert
        weight_all = lax.optimization_barrier(jnp.sum(jnp.where(hits, gate_weights, jnp.float32(0.0)), axis=1))
        routed = jnp.any(hits, axis=1)
        chosen = jnp.nonzero(routed, size=bound_rows, fill_value=0)[0].astype(jnp.int32)
        valid = (jnp.arange(bound_rows, dtype=jnp.int32) < jnp.sum(routed.astype(jnp.int32))).astype(jnp.float32)
        rows_in = normed[chosen]
        gate_sum = jnp.dot(rows_in, expert_gate[expert], preferred_element_type=jnp.float32)
        upward = jnp.dot(rows_in, expert_up[expert], preferred_element_type=jnp.float32)
        hidden = (jax.nn.silu(gate_sum) * upward).astype(jnp.bfloat16)
        result = jnp.dot(hidden, expert_down[expert], preferred_element_type=jnp.float32)
        scale_rows = weight_all[chosen] * valid
        totals = totals.at[chosen].add(result * scale_rows[:, None])
        return (totals, None)
    start_sum = jnp.zeros((TOKENS, D), jnp.float32)
    totals, _ = lax.scan(one_expert, start_sum, jnp.arange(EXPERTS, dtype=jnp.int32))
    return totals.astype(jnp.bfloat16)
```

```python
import functools

import jax
import jax.numpy as jnp
from jax import lax
from jax.experimental import pallas as pl
from jax.experimental.pallas import tpu as pltpu
from jax.sharding import PartitionSpec as P

MESH = pl.DeviceIdType.MESH
GROUPS = 4
NZ, NX, NY, NC = 8, 4, 4, 2
NE, NT = NZ * NX, NY * NC
CHUNKS = 4
PER = NE // CHUNKS
epsilon = 1e-05
F32, BF16 = jnp.float32, jnp.bfloat16


def offsets(n):
    q, r = n // PER, n % PER
    half, dx = r // NX, r % NX
    return q + half * (NZ - 1 - 2 * q), dx


def kernel(
    tokens_h, gain_v, shift_v, ids_v, gw_v, gate_h, up_h, down_h, out_v,
    tok, wall, packed, gath, wd, hid, outb, ret, combine,
    load_sem, disp_send, disp_recv, ag_send, ag_recv, wd_send, wd_recv, hid_send, hid_recv, ret_send, ret_recv,
):
    ep, tp = lax.axis_index("ep"), lax.axis_index("tp")
    ez, ex = ep // NX, ep % NX
    ty, tc = tp // NC, tp % NC
    mate = ty * NC + 1 - tc
    rows, features = tok.shape
    share = features // NT
    block = packed.shape[0] // NE
    half = wall.shape[1]

    def source_of(n):
        dz, dx = offsets(n)
        return ((ez + dz) % NZ) * NX + (ex + dx) % NX

    def dest_of(n):
        dz, dx = offsets(n)
        return ((ez + NZ - dz) % NZ) * NX + (ex + NX - dx) % NX

    barrier = pltpu.get_barrier_semaphore()

    @pl.loop(1, NE)
    def _(d):
        pl.semaphore_signal(barrier, inc=1, device_id=((ep + d) % NE, tp), device_id_type=MESH)

    @pl.loop(1, NT)
    def _(d):
        pl.semaphore_signal(barrier, inc=1, device_id=(ep, (tp + d) % NT), device_id_type=MESH)

    def tp_cols(t):
        return pl.ds(pl.multiple_of(t * share, share), share)

    load_tok = pltpu.make_async_copy(tokens_h, tok, load_sem.at[0])
    load_gate = pltpu.make_async_copy(gate_h, wall.at[pl.ds(0, 2)], load_sem.at[1])
    load_up = pltpu.make_async_copy(up_h, wall.at[pl.ds(2, 2)], load_sem.at[2])
    load_down = pltpu.make_async_copy(down_h.at[:, :, tp_cols(tp)], wd.at[tp], load_sem.at[3])
    load_tok.start()
    load_gate.start()
    load_up.start()
    load_down.start()

    experts = NE * (wall.shape[0] // 2)
    cap = NE * block // experts
    ids, gw = ids_v[...], gw_v[...]
    numbers = lax.broadcasted_iota(jnp.int32, (experts, rows), 0)
    hits = jnp.zeros((experts, rows), F32)
    weights = jnp.zeros((experts, rows), F32)
    for k in range(ids.shape[0]):
        same = ids[k : k + 1, :] == numbers
        hits = hits + jnp.where(same, 1.0, 0.0)
        weights = weights + jnp.where(same, gw[k : k + 1, :], 0.0)
    earlier = lax.broadcasted_iota(jnp.int32, (rows, rows), 0) < lax.broadcasted_iota(jnp.int32, (rows, rows), 1)
    before = jnp.dot(hits.astype(BF16), jnp.where(earlier, 1.0, 0.0).astype(BF16), preferred_element_type=F32)
    code = (hits * (before + 1.0)).astype(BF16)
    slots = experts * cap
    spread = (
        lax.broadcasted_iota(jnp.int32, (slots, experts), 0) // cap
        == lax.broadcasted_iota(jnp.int32, (slots, experts), 1)
    )
    spread_f = jnp.where(spread, 1.0, 0.0)
    wanted = (lax.broadcasted_iota(jnp.int32, (slots, rows), 0) % cap + 1).astype(F32)
    place = jnp.dot(spread_f.astype(BF16), code, preferred_element_type=F32) == wanted
    w_slots = jnp.dot(spread_f, weights, preferred_element_type=F32, precision=lax.Precision.HIGHEST)
    combine[...] = jnp.where(place, w_slots, 0.0).T

    load_tok.wait()
    values = tok[...].astype(F32)
    centre = jnp.mean(values, axis=-1, keepdims=True)
    spread_t = jnp.mean(jnp.square(values - centre), axis=-1, keepdims=True)
    own = tok[:, tp_cols(tp)].astype(F32)
    normed = (own - centre) * lax.rsqrt(spread_t + epsilon) * gain_v[:, tp_cols(tp)] + shift_v[:, tp_cols(tp)]
    normed = normed.astype(BF16)
    packed[...] = jnp.dot(jnp.where(place, 1.0, 0.0).astype(BF16), normed, preferred_element_type=F32).astype(BF16)
    gath[tp, 0, :block, :] = packed[pl.ds(pl.multiple_of(ep * block, block), block), :]

    pl.semaphore_wait(barrier, NE - 1 + NT - 1)

    @pl.loop(1, NE)
    def _(n):
        dest = dest_of(n)
        pltpu.make_async_remote_copy(
            src_ref=packed.at[pl.ds(pl.multiple_of(dest * block, block), block)],
            dst_ref=gath.at[tp, n // PER, pl.ds(pl.multiple_of((n % PER) * block, block), block)],
            send_sem=disp_send,
            recv_sem=disp_recv.at[n // PER],
            device_id=(dest, tp),
            device_id_type=MESH,
        ).start()

    @pl.loop(1, NT)
    def _(d):
        t = (tp + d) % NT
        pltpu.make_async_remote_copy(
            src_ref=down_h.at[:, :, tp_cols(t)],
            dst_ref=wd.at[tp],
            send_sem=wd_send,
            recv_sem=wd_recv,
            device_id=(ep, t),
            device_id_type=MESH,
        ).start()

    def arrived(ref, sem):
        pltpu.make_async_copy(ref, ref, sem).wait()

    def share_out(buf, slot, q, send, recv, t):
        pltpu.make_async_remote_copy(
            src_ref=buf.at[slot, q],
            dst_ref=buf.at[slot, q],
            send_sem=send,
            recv_sem=recv.at[slot, q],
            device_id=(ep, t),
            device_id_type=MESH,
        ).start()

    def spread_own(buf, q, send, recv):
        for dy in (2, 1, 3):
            share_out(buf, tp, q, send, recv, ((ty + dy) % NY) * NC + tc)
        share_out(buf, tp, q, send, recv, mate)

    def forward(buf, q, send, recv):
        for dy in (1, 3, 2):
            slot = ((ty + dy) % NY) * NC + tc
            arrived(buf.at[slot, q], recv.at[slot, q])
            share_out(buf, slot, q, send, recv, mate)

    def from_mate(buf, q, recv):
        for dy in (0, 1, 3, 2):
            slot = ((ty + dy) % NY) * NC + 1 - tc
            arrived(buf.at[slot, q], recv.at[slot, q])

    chunk_rows = PER * block

    def stage_a(q):
        if q == 0:
            part = gath.at[tp, 0, pl.ds(block, chunk_rows - block)]
        else:
            part = gath.at[tp, q]
        arrived(part, disp_recv.at[q])
        spread_own(gath, q, ag_send, ag_recv)

    def stage_b(q):
        forward(gath, q, ag_send, ag_recv)

    def stage_c(q):
        if q == 0:
            load_gate.wait()
            load_up.wait()
        from_mate(gath, q, ag_recv)
        x = jnp.concatenate([gath[s, q] for s in range(NT)], axis=-1)
        both = lax.dot_general(
            x, wall[...].reshape(4 * half, features), (((1,), (1,)), ((), ())), preferred_element_type=F32
        )
        g, u = both[:, : 2 * half], both[:, 2 * half :]
        h = g / (1.0 + jnp.exp(-g)) * u
        row = lax.broadcasted_iota(jnp.int32, h.shape, 0)
        lane = lax.broadcasted_iota(jnp.int32, h.shape, 1)
        hid[tp, q] = jnp.where((row % block) // cap == lane // half, h, 0.0).astype(BF16)
        spread_own(hid, q, hid_send, hid_recv)

    def stage_d(q):
        forward(hid, q, hid_send, hid_recv)

    def stage_e(q):
        if q == 0:
            load_down.wait()
            arrived(wd.at[pl.ds(0, NT - 1)], wd_recv)
        from_mate(hid, q, hid_recv)
        x = jnp.concatenate([hid[s, q] for s in range(NT)], axis=-1)
        result = jnp.dot(x, wd[...].reshape(NT * 2 * half, share), preferred_element_type=F32)
        outb[q] = result
        if q == 0:
            ret[ep] = result[:block]

        @pl.loop(1 if q == 0 else 0, PER)
        def _(r):
            dest = source_of(q * PER + r)
            pltpu.make_async_remote_copy(
                src_ref=outb.at[q, pl.ds(pl.multiple_of(r * block, block), block)],
                dst_ref=ret.at[ep],
                send_sem=ret_send,
                recv_sem=ret_recv,
                device_id=(dest, tp),
                device_id_type=MESH,
            ).start()

    stages = (stage_a, stage_b, stage_c, stage_d, stage_e)
    for step in range(CHUNKS + len(stages) - 1):
        for lag, stage in enumerate(stages):
            if 0 <= step - lag < CHUNKS:
                stage(step - lag)

    arrived(ret.at[pl.ds(0, NE - 1)], ret_recv)
    back = ret[...].reshape(NE * block, share)
    out_v[...] = jnp.dot(
        combine[...], back, preferred_element_type=F32, precision=lax.Precision.HIGHEST
    ).astype(BF16)

    arrived(packed.at[pl.ds(0, (NE - 1) * block)], disp_send)
    arrived(wd.at[pl.ds(0, NT - 1)], wd_send)
    arrived(gath.at[pl.ds(0, NT - 1)], ag_send)
    arrived(hid.at[pl.ds(0, NT - 1)], hid_send)
    arrived(ret.at[pl.ds(0, NE - 1)], ret_send)


def per_device(tokens, norm_gain, norm_shift, expert_ids, gate_weights, expert_gate, expert_up, expert_down):
    rows, features = tokens.shape
    local, _, half = expert_gate.shape
    share = features // NT
    cap = rows // 2 * expert_ids.shape[1] // (local * NE // GROUPS)
    block = local * cap
    any_spec = pl.BlockSpec(memory_space=pl.ANY)
    vmem = pl.BlockSpec(memory_space=pltpu.VMEM)
    dma = pltpu.SemaphoreType.DMA
    return pl.pallas_call(
        kernel,
        out_shape=jax.ShapeDtypeStruct((rows, share), BF16),
        in_specs=[any_spec, vmem, vmem, vmem, vmem, any_spec, any_spec, any_spec],
        out_specs=vmem,
        scratch_shapes=[
            pltpu.VMEM((rows, features), BF16),
            pltpu.VMEM((2 * local, half, features), BF16),
            pltpu.VMEM((NE * block, share), BF16),
            pltpu.VMEM((NT, CHUNKS, PER * block, share), BF16),
            pltpu.VMEM((NT, local, half, share), BF16),
            pltpu.VMEM((NT, CHUNKS, PER * block, local * half), BF16),
            pltpu.VMEM((CHUNKS, PER * block, share), F32),
            pltpu.VMEM((NE, block, share), F32),
            pltpu.VMEM((rows, NE * block), F32),
            dma((4,)),
            dma,
            dma((CHUNKS,)),
            dma,
            dma((NT, CHUNKS)),
            dma,
            dma,
            dma,
            dma((NT, CHUNKS)),
            dma,
            dma,
        ],
        compiler_params=pltpu.CompilerParams(
            collective_id=0, has_side_effects=True, vmem_limit_bytes=56 * 2**20
        ),
    )(
        tokens,
        norm_gain.reshape(1, features),
        norm_shift.reshape(1, features),
        expert_ids.T,
        gate_weights.T,
        expert_gate.transpose(0, 2, 1),
        expert_up.transpose(0, 2, 1),
        expert_down,
    )


def solution(mesh):
    return jax.shard_map(
        per_device,
        mesh=mesh,
        in_specs=(
            P("ep", None),
            P(),
            P(),
            P("ep", None),
            P("ep", None),
            P("ep", None, "tp"),
            P("ep", None, "tp"),
            P("ep", "tp", None),
        ),
        out_specs=P("ep", "tp"),
        check_vma=False,
    )
```

```python
import functools

import jax
import jax.numpy as jnp
from jax import lax
from jax.experimental import pallas as pl
from jax.experimental.pallas import tpu as pltpu
from jax.sharding import PartitionSpec as P

MESH = pl.DeviceIdType.MESH
GROUPS = 4
NZ, NX, NY, NC = 8, 4, 4, 2
NE, NT = NZ * NX, NY * NC
CHUNKS = 4
PER = NE // CHUNKS
epsilon = 1e-05
LEVELS = 32767.0
F32, BF16 = jnp.float32, jnp.bfloat16


def offsets(n):
    q, r = n // PER, n % PER
    half, dx = r // NX, r % NX
    return q + half * (NZ - 1 - 2 * q), dx


def kernel(
    tokens_h, gain_v, shift_v, ids_v, gw_v, gate_h, up_h, down_h, out_v,
    tok, wall, packed, gath, wd, hid, outb, outs, ret, rets, combine,
    load_sem, disp_send, disp_recv, ag_send, ag_recv, wd_send, wd_recv, hid_send, hid_recv, ret_send, ret_recv,
    rets_send, rets_recv,
):
    ep, tp = lax.axis_index("ep"), lax.axis_index("tp")
    ez, ex = ep // NX, ep % NX
    ty, tc = tp // NC, tp % NC
    mate = ty * NC + 1 - tc
    rows, features = tok.shape
    share = features // NT
    block = packed.shape[0] // NE
    half = wall.shape[1]

    def source_of(n):
        dz, dx = offsets(n)
        return ((ez + dz) % NZ) * NX + (ex + dx) % NX

    def dest_of(n):
        dz, dx = offsets(n)
        return ((ez + NZ - dz) % NZ) * NX + (ex + NX - dx) % NX

    barrier = pltpu.get_barrier_semaphore()

    @pl.loop(1, NE)
    def _(d):
        pl.semaphore_signal(barrier, inc=1, device_id=((ep + d) % NE, tp), device_id_type=MESH)

    @pl.loop(1, NT)
    def _(d):
        pl.semaphore_signal(barrier, inc=1, device_id=(ep, (tp + d) % NT), device_id_type=MESH)

    def tp_cols(t):
        return pl.ds(pl.multiple_of(t * share, share), share)

    load_tok = pltpu.make_async_copy(tokens_h, tok, load_sem.at[0])
    load_gate = pltpu.make_async_copy(gate_h, wall.at[pl.ds(0, 2)], load_sem.at[1])
    load_up = pltpu.make_async_copy(up_h, wall.at[pl.ds(2, 2)], load_sem.at[2])
    load_down = pltpu.make_async_copy(down_h.at[:, :, tp_cols(tp)], wd.at[tp], load_sem.at[3])
    load_tok.start()
    load_gate.start()
    load_up.start()
    load_down.start()

    experts = NE * (wall.shape[0] // 2)
    cap = NE * block // experts
    ids, gw = ids_v[...], gw_v[...]
    numbers = lax.broadcasted_iota(jnp.int32, (experts, rows), 0)
    hits = jnp.zeros((experts, rows), F32)
    weights = jnp.zeros((experts, rows), F32)
    for k in range(ids.shape[0]):
        same = ids[k : k + 1, :] == numbers
        hits = hits + jnp.where(same, 1.0, 0.0)
        weights = weights + jnp.where(same, gw[k : k + 1, :], 0.0)
    earlier = lax.broadcasted_iota(jnp.int32, (rows, rows), 0) < lax.broadcasted_iota(jnp.int32, (rows, rows), 1)
    before = jnp.dot(hits.astype(BF16), jnp.where(earlier, 1.0, 0.0).astype(BF16), preferred_element_type=F32)
    code = (hits * (before + 1.0)).astype(BF16)
    slots = experts * cap
    spread = (
        lax.broadcasted_iota(jnp.int32, (slots, experts), 0) // cap
        == lax.broadcasted_iota(jnp.int32, (slots, experts), 1)
    )
    spread_f = jnp.where(spread, 1.0, 0.0)
    wanted = (lax.broadcasted_iota(jnp.int32, (slots, rows), 0) % cap + 1).astype(F32)
    place = jnp.dot(spread_f.astype(BF16), code, preferred_element_type=F32) == wanted
    load_tok.wait()
    values = tok[...].astype(F32)
    centre = jnp.mean(values, axis=-1, keepdims=True)
    spread_t = jnp.mean(jnp.square(values - centre), axis=-1, keepdims=True)
    own = tok[:, tp_cols(tp)].astype(F32)
    normed = (own - centre) * lax.rsqrt(spread_t + epsilon) * gain_v[:, tp_cols(tp)] + shift_v[:, tp_cols(tp)]
    normed = normed.astype(BF16)
    packed[...] = jnp.dot(jnp.where(place, 1.0, 0.0).astype(BF16), normed, preferred_element_type=F32).astype(BF16)
    gath[tp, 0, :block, :] = packed[pl.ds(pl.multiple_of(ep * block, block), block), :]

    with jax.named_scope("entry_wait"):
        pl.semaphore_wait(barrier, NE - 1 + NT - 1)

    @pl.loop(1, NE)
    def _(n):
        dest = dest_of(n)
        pltpu.make_async_remote_copy(
            src_ref=packed.at[pl.ds(pl.multiple_of(dest * block, block), block)],
            dst_ref=gath.at[tp, n // PER, pl.ds(pl.multiple_of((n % PER) * block, block), block)],
            send_sem=disp_send,
            recv_sem=disp_recv.at[n // PER],
            device_id=(dest, tp),
            device_id_type=MESH,
        ).start()

    @pl.loop(1, NT)
    def _(d):
        t = (tp + d) % NT
        pltpu.make_async_remote_copy(
            src_ref=down_h.at[:, :, tp_cols(t)],
            dst_ref=wd.at[tp],
            send_sem=wd_send,
            recv_sem=wd_recv,
            device_id=(ep, t),
            device_id_type=MESH,
        ).start()

    w_slots = jnp.dot(spread_f, weights, preferred_element_type=F32, precision=lax.Precision.HIGHEST)
    combine[...] = jnp.where(place, w_slots, 0.0).T

    def arrived(ref, sem):
        pltpu.make_async_copy(ref, ref, sem).wait()

    def share_out(buf, slot, q, send, recv, t, part=None):
        ref = buf.at[slot, q] if part is None else buf.at[slot, q, part]
        pltpu.make_async_remote_copy(
            src_ref=ref,
            dst_ref=ref,
            send_sem=send,
            recv_sem=recv.at[slot, q],
            device_id=(ep, t),
            device_id_type=MESH,
        ).start()

    def along(dy):
        return ((ty + dy) % NY) * NC + tc

    def from_mate(buf, q, recv):
        for dy in (0, 1, 3, 2):
            slot = ((ty + dy) % NY) * NC + 1 - tc
            arrived(buf.at[slot, q], recv.at[slot, q])

    chunk_rows = PER * block

    halves = (pl.ds(0, chunk_rows // 2), pl.ds(chunk_rows // 2, chunk_rows // 2))

    def stage_a(q):
        if q == 0:
            part = gath.at[tp, 0, pl.ds(block, chunk_rows - block)]
        else:
            part = gath.at[tp, q]
        arrived(part, disp_recv.at[q])
        share_out(gath, tp, q, ag_send, ag_recv, along(1))
        share_out(gath, tp, q, ag_send, ag_recv, along(3))
        share_out(gath, tp, q, ag_send, ag_recv, mate)

    def stage_b(q):
        for here, there, part in ((3, 1, halves[0]), (1, 3, halves[1])):
            arrived(gath.at[along(here), q], ag_recv.at[along(here), q])
            share_out(gath, along(here), q, ag_send, ag_recv, along(there), part)
            share_out(gath, along(here), q, ag_send, ag_recv, mate)

    def stage_c(q):
        arrived(gath.at[along(2), q], ag_recv.at[along(2), q])
        share_out(gath, along(2), q, ag_send, ag_recv, mate)

    def stage_d(q):
        if q == 0:
            load_gate.wait()
            load_up.wait()
        from_mate(gath, q, ag_recv)
        x = jnp.concatenate([gath[s, q] for s in range(NT)], axis=-1)
        both = lax.dot_general(
            x, wall[...].reshape(4 * half, features), (((1,), (1,)), ((), ())), preferred_element_type=F32
        )
        g, u = both[:, : 2 * half], both[:, 2 * half :]
        h = (g / (1.0 + jnp.exp(-g)) * u).reshape(PER, 2, cap, 2 * half)
        lane = lax.broadcasted_iota(jnp.int32, (PER, cap, 2 * half), 2)
        h = jnp.where(lane < half, h[:, 0], h[:, 1])
        hid[tp, q] = h.reshape(PER * cap, 2 * half).astype(BF16)
        for dy in (2, 1, 3):
            share_out(hid, tp, q, hid_send, hid_recv, along(dy))
        share_out(hid, tp, q, hid_send, hid_recv, mate)

    def stage_e(q):
        for dy in (1, 3, 2):
            arrived(hid.at[along(dy), q], hid_recv.at[along(dy), q])
            share_out(hid, along(dy), q, hid_send, hid_recv, mate)

    def stage_f(q):
        if q == 0:
            load_down.wait()
            arrived(wd.at[pl.ds(0, NT - 1)], wd_recv)
        from_mate(hid, q, hid_recv)
        lane = lax.broadcasted_iota(jnp.int32, (PER, cap, 2 * half), 2)
        parts = []
        for s in range(NT):
            h = hid[s, q].astype(F32).reshape(PER, cap, 2 * half)
            pair = jnp.stack([jnp.where(lane < half, h, 0.0), jnp.where(lane < half, 0.0, h)], axis=1)
            parts.append(pair.reshape(chunk_rows, 2 * half).astype(BF16))
        x = jnp.concatenate(parts, axis=-1)
        result = jnp.dot(x, wd[...].reshape(NT * 2 * half, share), preferred_element_type=F32)
        top = jnp.maximum(jnp.max(jnp.abs(result), axis=-1, keepdims=True), 1e-30)
        level = jnp.round(result * (LEVELS / top)).astype(jnp.int32)
        outb[q] = level.astype(jnp.int16)
        row = lax.broadcasted_iota(jnp.int32, (chunk_rows, 128), 0) % block
        col = lax.broadcasted_iota(jnp.int32, (chunk_rows, 128), 1)
        scales = jnp.where(col == row + (ep % (128 // block)) * block, top * (1.0 / LEVELS), 0.0)
        outs[q] = jnp.sum(scales.reshape(PER, block, 128), axis=1, keepdims=True)
        if q == 0:
            ret[ep] = outb[0, 0:block]
            rets[ep] = outs[0, 0]

        @pl.loop(1 if q == 0 else 0, PER)
        def _(r):
            dest = source_of(q * PER + r)
            pltpu.make_async_remote_copy(
                src_ref=outb.at[q, pl.ds(pl.multiple_of(r * block, block), block)],
                dst_ref=ret.at[ep],
                send_sem=ret_send,
                recv_sem=ret_recv,
                device_id=(dest, tp),
                device_id_type=MESH,
            ).start()
            pltpu.make_async_remote_copy(
                src_ref=outs.at[q, r],
                dst_ref=rets.at[ep],
                send_sem=rets_send,
                recv_sem=rets_recv,
                device_id=(dest, tp),
                device_id_type=MESH,
            ).start()

    stages = (stage_a, stage_b, stage_c, stage_d, stage_e, stage_f)
    for step in range(CHUNKS + len(stages) - 1):
        for lag, stage in enumerate(stages):
            if 0 <= step - lag < CHUNKS:
                with jax.named_scope(f"{stage.__name__}{step - lag}"):
                    stage(step - lag)

    with jax.named_scope("ret_wait"):
        arrived(ret.at[pl.ds(0, NE - 1)], ret_recv)
    arrived(rets.at[pl.ds(0, NE - 1)], rets_recv)
    per = 128 // block
    scale = jnp.concatenate([jnp.sum(rets[pl.ds(i * per, per)], axis=0) for i in range(NE // per)], axis=-1)
    back = ret[...].astype(jnp.int32).astype(F32).reshape(NE * block, share)
    out_v[...] = jnp.dot(
        combine[...] * scale, back, preferred_element_type=F32, precision=lax.Precision.HIGHEST
    ).astype(BF16)

    arrived(packed.at[pl.ds(0, (NE - 1) * block)], disp_send)
    arrived(wd.at[pl.ds(0, NT - 1)], wd_send)
    arrived(gath.at[pl.ds(0, NT - 1)], ag_send)
    arrived(hid.at[pl.ds(0, NT - 1)], hid_send)
    arrived(ret.at[pl.ds(0, NE - 1)], ret_send)
    arrived(rets.at[pl.ds(0, NE - 1)], rets_send)


def per_device(tokens, norm_gain, norm_shift, expert_ids, gate_weights, expert_gate, expert_up, expert_down):
    rows, features = tokens.shape
    local, _, half = expert_gate.shape
    share = features // NT
    cap = rows // 2 * expert_ids.shape[1] // (local * NE // GROUPS)
    block = local * cap
    any_spec = pl.BlockSpec(memory_space=pl.ANY)
    vmem = pl.BlockSpec(memory_space=pltpu.VMEM)
    dma = pltpu.SemaphoreType.DMA
    return pl.pallas_call(
        kernel,
        out_shape=jax.ShapeDtypeStruct((rows, share), BF16),
        in_specs=[any_spec, vmem, vmem, vmem, vmem, any_spec, any_spec, any_spec],
        out_specs=vmem,
        scratch_shapes=[
            pltpu.VMEM((rows, features), BF16),
            pltpu.VMEM((2 * local, half, features), BF16),
            pltpu.VMEM((NE * block, share), BF16),
            pltpu.VMEM((NT, CHUNKS, PER * block, share), BF16),
            pltpu.VMEM((NT, local, half, share), BF16),
            pltpu.VMEM((NT, CHUNKS, PER * cap, local * half), BF16),
            pltpu.VMEM((CHUNKS, PER * block, share), jnp.int16),
            pltpu.VMEM((CHUNKS, PER, 1, 128), F32),
            pltpu.VMEM((NE, block, share), jnp.int16),
            pltpu.VMEM((NE, 1, 128), F32),
            pltpu.VMEM((rows, NE * block), F32),
            dma((4,)),
            dma,
            dma((CHUNKS,)),
            dma,
            dma((NT, CHUNKS)),
            dma,
            dma,
            dma,
            dma((NT, CHUNKS)),
            dma,
            dma,
            dma,
            dma,
        ],
        compiler_params=pltpu.CompilerParams(
            collective_id=0, has_side_effects=True, vmem_limit_bytes=56 * 2**20
        ),
    )(
        tokens,
        norm_gain.reshape(1, features),
        norm_shift.reshape(1, features),
        expert_ids.T,
        gate_weights.T,
        expert_gate.transpose(0, 2, 1),
        expert_up.transpose(0, 2, 1),
        expert_down,
    )


def solution(mesh):
    return jax.shard_map(
        per_device,
        mesh=mesh,
        in_specs=(
            P("ep", None),
            P(),
            P(),
            P("ep", None),
            P("ep", None),
            P("ep", None, "tp"),
            P("ep", None, "tp"),
            P("ep", "tp", None),
        ),
        out_specs=P("ep", "tp"),
        check_vma=False,
    )
```

```python
import jax
import jax.numpy as jnp
from jax import lax
from jax.experimental import pallas as pl
from jax.experimental.pallas import tpu as pltpu
from jax.sharding import PartitionSpec as P

MESH = pl.DeviceIdType.MESH
GROUPS = 4
NZ, NX, NY, NC = 8, 4, 4, 2
NE, NT = NZ * NX, NY * NC
ABSOLUTE = 2
SEND_FAR = True
SIG_FAR = True
ORDER = (0, 7, 1, 6, 2, 5, 3, 4)
CHUNKS = 4
LINES = NZ // CHUNKS
PER = NE // CHUNKS
RELAY = True
SEQ = ("a0", "a1", "a2", "a3", "b0", "b1", "b2", "b3", "d0", "d1", "d2", "d3", "f0", "f1", "f2", "f3")
FINAL_CAST = True
VMEM_LIMIT = 56 * 2**20
epsilon = 1e-05
LEVELS = 32767.0
F32, BF16 = jnp.float32, jnp.bfloat16


def kernel(
    tokens_h, gain_v, shift_v, ids_v, gw_v, gate_h, up_h, down_h, out_v,
    tok, wall, packed, gath, wd, hid, outb, outs, ret, rets, combine,
    load_sem, disp_send, disp_recv, ag_send, ag_recv, wall_send, wall_recv, wd_send, wd_recv, hid_send, hid_recv,
    ret_send, ret_recv, rets_send, rets_recv,
):
    ep, tp = lax.axis_index("ep"), lax.axis_index("tp")
    ez, ex = ep // NX, ep % NX
    ty, tc = tp // NC, tp % NC
    mate = ty * NC + 1 - tc
    rows, features = tok.shape
    quarter = features // NY
    share = quarter // NC
    block = packed.shape[0] // NE
    cap = block // NC
    half = wall.shape[2]
    chunk_rows = PER * block
    work_rows = PER * cap
    own_line = (ORDER.index(0), ez, ez % 4 * 2 + ez // 4, ez // 4 * 4 + ez % 2 * 2 + ez % 4 // 2)[ABSOLUTE]
    own_q = own_line // LINES

    def arrived(ref, sem):
        pltpu.make_async_copy(ref, ref, sem).wait()

    def send(src, dst, send_sem, recv_sem, e, t):
        pltpu.make_async_remote_copy(
            src_ref=src, dst_ref=dst, send_sem=send_sem, recv_sem=recv_sem, device_id=(e, t), device_id_type=MESH
        ).start()

    def rows_of(n):
        return pl.ds(pl.multiple_of(n * block, block), block)

    def quarter_of(y):
        return pl.ds(pl.multiple_of(y * quarter, quarter), quarter)

    load_tok = pltpu.make_async_copy(tokens_h, tok, load_sem.at[0])
    load_gate = pltpu.make_async_copy(gate_h.at[tc], wall.at[0, tc], load_sem.at[1])
    load_up = pltpu.make_async_copy(up_h.at[tc], wall.at[1, tc], load_sem.at[2])
    load_down = pltpu.make_async_copy(down_h.at[tc, :, quarter_of(ty)], wd.at[tp], load_sem.at[3])
    load_tok.start()

    barrier = pltpu.get_barrier_semaphore()

    def signal(e, t):
        pl.semaphore_signal(barrier, inc=1, device_id=(e, t), device_id_type=MESH)

    for dz in (4, 3, 5, 2, 6, 1, 7, 0):
        for dx in range(1 if dz == 0 else 0, NX):
            signal(((ez + dz) % NZ) * NX + (ex + dx) % NX, tp)
    for d in range(1, NT):
        signal(ep, (tp + d) % NT)

    ids, gw = ids_v[...], gw_v[...]
    earlier = lax.broadcasted_iota(jnp.int32, (rows, rows), 0) < lax.broadcasted_iota(jnp.int32, (rows, rows), 1)
    earlier = jnp.where(earlier, 1.0, 0.0).astype(BF16)

    def placed(numbers):
        hits = jnp.zeros(numbers.shape, F32)
        weights = jnp.zeros(numbers.shape, F32)
        for k in range(ids.shape[0]):
            same = ids[k : k + 1, :] == numbers
            hits = hits + jnp.where(same, 1.0, 0.0)
            weights = weights + jnp.where(same, gw[k : k + 1, :], 0.0)
        before = jnp.dot(hits.astype(BF16), earlier, preferred_element_type=F32)
        code = hits * (before + 1.0)
        wanted = (lax.broadcasted_iota(jnp.int32, (numbers.shape[0], cap, rows), 1) + 1).astype(F32)
        return code[:, None, :] == wanted, weights

    with jax.named_scope("p_place"):
        place, _ = placed(lax.broadcasted_iota(jnp.int32, (NE, rows), 0) * NC + tc)
        place = jnp.where(place, 1.0, 0.0).reshape(NE * cap, rows).astype(BF16)

    load_tok.wait()
    load_gate.start()
    load_up.start()
    load_down.start()
    with jax.named_scope("p_ln"):
        values = tok[...].astype(F32)
        centre = jnp.mean(values, axis=-1, keepdims=True)
        spread = jnp.mean(jnp.square(values - centre), axis=-1, keepdims=True)
        own = tok[:, quarter_of(ty)].astype(F32)
        normed = (own - centre) * lax.rsqrt(spread + epsilon) * gain_v[:, quarter_of(ty)] + shift_v[:, quarter_of(ty)]
        picked = jnp.dot(place, normed.astype(BF16), preferred_element_type=F32).reshape(NE, cap, quarter)
        picked = jnp.stack([picked[:, :, :share], picked[:, :, share:]], axis=1)
        packed[...] = picked.reshape(NE * block, share).astype(BF16)
        gath[ty, own_q, rows_of(own_line % LINES * NX + ex), :] = packed[rows_of(ep), :]

    with jax.named_scope("entry_wait"):
        pl.semaphore_wait(barrier, NE - 1 + NT - 1)

    sends = tuple(enumerate(ORDER))
    for line, dz in reversed(sends) if SEND_FAR else sends:
        line = own_line if ABSOLUTE else line

        @pl.loop(1 if dz == 0 else 0, NX)
        def _(dx):
            e = ((ez + NZ - dz) % NZ) * NX + (ex + dx) % NX
            send(
                packed.at[rows_of(e)], gath.at[ty, line // LINES, rows_of(line % LINES * NX + ex)],
                disp_send, disp_recv.at[line // LINES], e, tp,
            )

    for d in range(1, NT):
        t = (tp + d) % NT
        send(down_h.at[t % NC, :, quarter_of(t // NC)], wd.at[tp], wd_send, wd_recv, ep, t)

    send(gate_h.at[1 - tc], wall.at[0, tc], wall_send, wall_recv, ep, mate)
    send(up_h.at[1 - tc], wall.at[1, tc], wall_send, wall_recv, ep, mate)

    with jax.named_scope("p_combine"):
        place, weights = placed(lax.broadcasted_iota(jnp.int32, (NE * NC, rows), 0))
        w_slots = jnp.where(place, weights[:, None, :], 0.0).reshape(NE * block, rows)
        combine[...] = w_slots.T

    def share_out(buf, y, q, send_sem, recv_sem, to, part=None):
        ref = buf.at[y, q] if part is None else buf.at[y, q, part]
        send(ref, ref, send_sem, recv_sem, ep, to * NC + tc)

    def along(dy):
        return (ty + dy) % NY

    halves = (pl.ds(0, chunk_rows // 2), pl.ds(chunk_rows // 2, chunk_rows // 2))

    def stage_a(q):
        @pl.when(own_q == q)
        def _():
            arrived(gath.at[ty, q, pl.ds(0, chunk_rows - block)], disp_recv.at[q])

        @pl.when(own_q != q)
        def _():
            arrived(gath.at[ty, q], disp_recv.at[q])

        if not RELAY:
            share_out(gath, ty, q, ag_send, ag_recv.at[ty, q], along(2))
        share_out(gath, ty, q, ag_send, ag_recv.at[ty, q], along(1))
        share_out(gath, ty, q, ag_send, ag_recv.at[ty, q], along(3))

    def stage_b(q):
        for here, there, part in ((3, 1, halves[0]), (1, 3, halves[1])):
            arrived(gath.at[along(here), q], ag_recv.at[along(here), q])
            if RELAY:
                share_out(gath, along(here), q, ag_send, ag_recv.at[along(here), q], along(there), part)

    def stage_d(q):
        if q == 0:
            load_gate.wait()
            load_up.wait()
            arrived(wall.at[0], wall_recv)
        arrived(gath.at[along(2), q], ag_recv.at[along(2), q])
        parts = []
        for y in range(NY):
            both = gath[y, q].astype(F32).reshape(PER, NC, cap, share)
            parts += [both[:, i].reshape(work_rows, share).astype(BF16) for i in range(NC)]
        x = jnp.concatenate(parts, axis=-1)
        both = lax.dot_general(
            x, wall[...].reshape(2 * NC * half, features), (((1,), (1,)), ((), ())), preferred_element_type=F32
        )
        g, u = both[:, : NC * half], both[:, NC * half :]
        hid[ty, q] = (g / (1.0 + jnp.exp(-g)) * u).astype(BF16)
        for dy in (2, 1, 3):
            share_out(hid, ty, q, hid_send, hid_recv.at[q], along(dy))

    def stage_f(q):
        if q == 0:
            load_down.wait()
            arrived(wd.at[pl.ds(0, NT - 1)], wd_recv)
        arrived(hid.at[pl.ds(0, NY - 1), q], hid_recv.at[q])
        x = jnp.concatenate([hid[y, q] for y in range(NY)], axis=-1)
        result = jnp.dot(x, wd[...].reshape(NT * half, quarter), preferred_element_type=F32)
        top = jnp.maximum(jnp.max(jnp.abs(result), axis=-1, keepdims=True), 1e-30)
        level = jnp.round(result * (LEVELS / top)).astype(jnp.int32)
        tiles = [level[:, i : i + 128].reshape(PER, cap, 128) for i in range(0, quarter, 128)]
        outb[q] = jnp.stack(tiles, axis=1).reshape(PER, NC, block, 128).astype(jnp.int16)
        row = lax.broadcasted_iota(jnp.int32, (work_rows, 128), 0) % cap
        col = lax.broadcasted_iota(jnp.int32, (work_rows, 128), 1)
        scales = jnp.where(col == row + tc * cap + ep % (128 // block) * block, top * (1.0 / LEVELS), 0.0)
        outs[q] = jnp.sum(scales.reshape(PER, cap, 128), axis=1, keepdims=True)

        @pl.when(own_q == q)
        def _():
            r = own_line % LINES * NX + ex
            ret[ep * NC + tc] = outb[q, r, tc]
            rets[ep * NC + tc] = outs[q, r]

        for k in range(LINES):
            line = q * LINES + k
            z = ((ez + ORDER[line]) % NZ, line, line // 2 + line % 2 * 4, line // 4 * 4 + line % 2 * 2 + line % 4 // 2)[ABSOLUTE]

            @pl.loop(0, NX)
            def _(x):
                e, r = z * NX + x, k * NX + x
                for c in range(NC):

                    @pl.when((e != ep) | (c != tc))
                    def _():
                        t = ty * NC + c
                        send(outb.at[q, r, c], ret.at[ep * NC + tc], ret_send, ret_recv, e, t)
                        send(outs.at[q, r], rets.at[ep * NC + tc], rets_send, rets_recv, e, t)

    stages = {"a": stage_a, "b": stage_b, "d": stage_d, "f": stage_f}
    for word in SEQ:
        with jax.named_scope(f"stage_{word}"):
            stages[word[0]](int(word[1:]))

    with jax.named_scope("ret_wait"):
        arrived(ret.at[pl.ds(0, NE * NC - 1)], ret_recv)
        arrived(rets.at[pl.ds(0, NE * NC - 1)], rets_recv)
    per = 128 // block
    scale = jnp.concatenate(
        [jnp.sum(rets[pl.ds(i * per * NC, per * NC)], axis=0) for i in range(NE // per)], axis=-1
    )
    back = ret[...].astype(jnp.int32).astype(F32).reshape(NE, NC, share // 128, cap, 128)
    back = jnp.concatenate([back[:, :, i].reshape(NE * block, 128) for i in range(share // 128)], axis=-1)
    out_v[...] = jnp.dot(
        combine[...] * scale, back, preferred_element_type=F32, precision=lax.Precision.HIGHEST
    ).astype(out_v.dtype)

    with jax.named_scope("drain"):
        arrived(packed.at[pl.ds(0, (NE - 1) * block)], disp_send)
        arrived(wd.at[pl.ds(0, NT - 1)], wd_send)
        arrived(wall.at[0], wall_send)
        arrived(gath.at[pl.ds(0, NY - 1)], ag_send)
        arrived(hid.at[pl.ds(0, NY - 1)], hid_send)
        arrived(ret.at[pl.ds(0, NE * NC - 1)], ret_send)
        arrived(rets.at[pl.ds(0, NE * NC - 1)], rets_send)


def per_device(tokens, norm_gain, norm_shift, expert_ids, gate_weights, expert_gate, expert_up, expert_down):
    rows, features = tokens.shape
    local, _, half = expert_gate.shape
    quarter = features // NY
    share = features // NT
    cap = rows // 2 * expert_ids.shape[1] // (local * NE // GROUPS)
    block = local * cap
    any_spec = pl.BlockSpec(memory_space=pl.ANY)
    vmem = pl.BlockSpec(memory_space=pltpu.VMEM)
    dma = pltpu.SemaphoreType.DMA
    out = pl.pallas_call(
        kernel,
        out_shape=jax.ShapeDtypeStruct((rows, share), F32 if FINAL_CAST else BF16),
        in_specs=[any_spec, vmem, vmem, vmem, vmem, any_spec, any_spec, any_spec],
        out_specs=vmem,
        scratch_shapes=[
            pltpu.VMEM((rows, features), BF16),
            pltpu.VMEM((2, NC, half, features), BF16),
            pltpu.VMEM((NE * block, share), BF16),
            pltpu.VMEM((NY, CHUNKS, PER * block, share), BF16),
            pltpu.VMEM((NT, half, quarter), BF16),
            pltpu.VMEM((NY, CHUNKS, PER * cap, NC * half), BF16),
            pltpu.VMEM((CHUNKS, PER, NC, block, 128), jnp.int16),
            pltpu.VMEM((CHUNKS, PER, 1, 128), F32),
            pltpu.VMEM((NE * NC, block, 128), jnp.int16),
            pltpu.VMEM((NE * NC, 1, 128), F32),
            pltpu.VMEM((rows, NE * block), F32),
            dma((4,)),
            dma,
            dma((CHUNKS,)),
            dma,
            dma((NY, CHUNKS)),
            dma,
            dma,
            dma,
            dma,
            dma,
            dma((CHUNKS,)),
            dma,
            dma,
            dma,
            dma,
        ],
        compiler_params=pltpu.CompilerParams(collective_id=0, has_side_effects=True, vmem_limit_bytes=VMEM_LIMIT),
    )(
        tokens,
        norm_gain.reshape(1, features),
        norm_shift.reshape(1, features),
        expert_ids.T,
        gate_weights.T,
        expert_gate.transpose(0, 2, 1),
        expert_up.transpose(0, 2, 1),
        expert_down,
    )
    return out.astype(BF16)


def solution(mesh):
    return jax.shard_map(
        per_device,
        mesh=mesh,
        in_specs=(
            P("ep", None),
            P(),
            P(),
            P("ep", None),
            P("ep", None),
            P("ep", None, "tp"),
            P("ep", None, "tp"),
            P("ep", "tp", None),
        ),
        out_specs=P("ep", "tp"),
        check_vma=False,
    )
```

```python
import jax
import jax.numpy as jnp
from jax import lax
from jax.experimental import pallas as pl
from jax.experimental.pallas import tpu as pltpu
from jax.sharding import PartitionSpec as P

MESH = pl.DeviceIdType.MESH
GROUPS = 4
NZ, NX, NY, NC = 8, 4, 4, 2
NE, NT = NZ * NX, NY * NC
ABSOLUTE = True
ZORDER = (0, 1, 2, 3, 4, 5, 6, 7)
SEND_FAR = True
SIG_FAR = True
ORDER = (0, 7, 1, 6, 2, 5, 3, 4)
CHUNKS = 4
LINES = NZ // CHUNKS
PER = NE // CHUNKS
RELAY = True
SEQ = ("a0", "a1", "a2", "a3", "b0", "b1", "b2", "b3", "d0", "d1", "d2", "d3", "f0", "f1", "f2", "f3")
FINAL_CAST = True
VMEM_LIMIT = 56 * 2**20
epsilon = 1e-05
LEVELS = 32760.0
KEYS = 128.0
F32, BF16 = jnp.float32, jnp.bfloat16


def kernel(
    tokens_h, gain_v, shift_v, ids_v, gw_v, gate_h, up_h, down_h, out_v,
    tok, wall, packed, gath, wd, hid, outb, ret, combine,
    load_sem, disp_send, disp_recv, ag_send, ag_recv, wall_send, wall_recv, wd_send, wd_recv, hid_send, hid_recv,
    ret_send, ret_recv,
):
    ep, tp = lax.axis_index("ep"), lax.axis_index("tp")
    ez, ex = ep // NX, ep % NX
    ty, tc = tp // NC, tp % NC
    mate = ty * NC + 1 - tc
    rows, features = tok.shape
    quarter = features // NY
    share = quarter // NC
    block = packed.shape[0] // NE
    cap = block // NC
    half = wall.shape[2]
    chunk_rows = PER * block
    work_rows = PER * cap
    own_line = sum(jnp.where(ez == z, line, 0) for line, z in enumerate(ZORDER)) if ABSOLUTE else ORDER.index(0)
    own_q = own_line // LINES

    def arrived(ref, sem):
        pltpu.make_async_copy(ref, ref, sem).wait()

    def send(src, dst, send_sem, recv_sem, e, t):
        pltpu.make_async_remote_copy(
            src_ref=src, dst_ref=dst, send_sem=send_sem, recv_sem=recv_sem, device_id=(e, t), device_id_type=MESH
        ).start()

    def rows_of(n):
        return pl.ds(pl.multiple_of(n * block, block), block)

    def quarter_of(y):
        return pl.ds(pl.multiple_of(y * quarter, quarter), quarter)

    load_tok = pltpu.make_async_copy(tokens_h, tok, load_sem.at[0])
    load_gate = pltpu.make_async_copy(gate_h.at[tc], wall.at[0, tc], load_sem.at[1])
    load_up = pltpu.make_async_copy(up_h.at[tc], wall.at[1, tc], load_sem.at[2])
    load_down = pltpu.make_async_copy(down_h.at[tc, :, quarter_of(ty)], wd.at[tp], load_sem.at[3])
    load_tok.start()

    barrier = pltpu.get_barrier_semaphore()

    def signal(e, t):
        pl.semaphore_signal(barrier, inc=1, device_id=(e, t), device_id_type=MESH)

    for dz in (4, 3, 5, 2, 6, 1, 7, 0):
        for dx in range(1 if dz == 0 else 0, NX):
            signal(((ez + dz) % NZ) * NX + (ex + dx) % NX, tp)
    for d in range(1, NT):
        signal(ep, (tp + d) % NT)

    ids, gw = ids_v[...], gw_v[...]
    earlier = lax.broadcasted_iota(jnp.int32, (rows, rows), 0) < lax.broadcasted_iota(jnp.int32, (rows, rows), 1)
    earlier = jnp.where(earlier, 1.0, 0.0).astype(BF16)

    def placed(numbers):
        hits = jnp.zeros(numbers.shape, F32)
        weights = jnp.zeros(numbers.shape, F32)
        for k in range(ids.shape[0]):
            same = ids[k : k + 1, :] == numbers
            hits = hits + jnp.where(same, 1.0, 0.0)
            weights = weights + jnp.where(same, gw[k : k + 1, :], 0.0)
        before = jnp.dot(hits.astype(BF16), earlier, preferred_element_type=F32)
        code = hits * (before + 1.0)
        wanted = (lax.broadcasted_iota(jnp.int32, (numbers.shape[0], cap, rows), 1) + 1).astype(F32)
        return code[:, None, :] == wanted, weights

    with jax.named_scope("p_place"):
        place, _ = placed(lax.broadcasted_iota(jnp.int32, (NE, rows), 0) * NC + tc)
        place = jnp.where(place, 1.0, 0.0).reshape(NE * cap, rows).astype(BF16)

    load_tok.wait()
    load_gate.start()
    load_up.start()
    load_down.start()
    with jax.named_scope("p_ln"):
        values = tok[...].astype(F32)
        centre = jnp.mean(values, axis=-1, keepdims=True)
        spread = jnp.mean(jnp.square(values - centre), axis=-1, keepdims=True)
        own = tok[:, quarter_of(ty)].astype(F32)
        normed = (own - centre) * lax.rsqrt(spread + epsilon) * gain_v[:, quarter_of(ty)] + shift_v[:, quarter_of(ty)]
        picked = jnp.dot(place, normed.astype(BF16), preferred_element_type=F32).reshape(NE, cap, quarter)
        picked = jnp.stack([picked[:, :, :share], picked[:, :, share:]], axis=1)
        packed[...] = picked.reshape(NE * block, share).astype(BF16)
        gath[ty, own_q, rows_of(own_line % LINES * NX + ex), :] = packed[rows_of(ep), :]

    with jax.named_scope("entry_wait"):
        pl.semaphore_wait(barrier, NE - 1 + NT - 1)

    sends = tuple(enumerate(ORDER))
    for line, dz in reversed(sends) if SEND_FAR else sends:
        line = own_line if ABSOLUTE else line

        @pl.loop(1 if dz == 0 else 0, NX)
        def _(dx):
            e = ((ez + NZ - dz) % NZ) * NX + (ex + dx) % NX
            send(
                packed.at[rows_of(e)], gath.at[ty, line // LINES, rows_of(line % LINES * NX + ex)],
                disp_send, disp_recv.at[line // LINES], e, tp,
            )

    for d in range(1, NT):
        t = (tp + d) % NT
        send(down_h.at[t % NC, :, quarter_of(t // NC)], wd.at[tp], wd_send, wd_recv, ep, t)

    send(gate_h.at[1 - tc], wall.at[0, tc], wall_send, wall_recv, ep, mate)
    send(up_h.at[1 - tc], wall.at[1, tc], wall_send, wall_recv, ep, mate)

    with jax.named_scope("p_combine"):
        place, weights = placed(lax.broadcasted_iota(jnp.int32, (NE * NC, rows), 0))
        w_slots = jnp.where(place, weights[:, None, :], 0.0).reshape(NE * block, rows)
        combine[...] = w_slots.T

    def share_out(buf, y, q, send_sem, recv_sem, to, part=None):
        ref = buf.at[y, q] if part is None else buf.at[y, q, part]
        send(ref, ref, send_sem, recv_sem, ep, to * NC + tc)

    def along(dy):
        return (ty + dy) % NY

    halves = (pl.ds(0, chunk_rows // 2), pl.ds(chunk_rows // 2, chunk_rows // 2))

    def stage_a(q):
        @pl.when(own_q == q)
        def _():
            arrived(gath.at[ty, q, pl.ds(0, chunk_rows - block)], disp_recv.at[q])

        @pl.when(own_q != q)
        def _():
            arrived(gath.at[ty, q], disp_recv.at[q])

        if not RELAY:
            share_out(gath, ty, q, ag_send, ag_recv.at[ty, q], along(2))
        share_out(gath, ty, q, ag_send, ag_recv.at[ty, q], along(1))
        share_out(gath, ty, q, ag_send, ag_recv.at[ty, q], along(3))

    def stage_b(q):
        for here, there, part in ((3, 1, halves[0]), (1, 3, halves[1])):
            arrived(gath.at[along(here), q], ag_recv.at[along(here), q])
            if RELAY:
                share_out(gath, along(here), q, ag_send, ag_recv.at[along(here), q], along(there), part)

    def stage_d(q):
        if q == 0:
            load_gate.wait()
            load_up.wait()
            arrived(wall.at[0], wall_recv)
        arrived(gath.at[along(2), q], ag_recv.at[along(2), q])
        parts = []
        for y in range(NY):
            both = gath[y, q].astype(F32).reshape(PER, NC, cap, share)
            parts += [both[:, i].reshape(work_rows, share).astype(BF16) for i in range(NC)]
        x = jnp.concatenate(parts, axis=-1)
        both = lax.dot_general(
            x, wall[...].reshape(2 * NC * half, features), (((1,), (1,)), ((), ())), preferred_element_type=F32
        )
        g, u = both[:, : NC * half], both[:, NC * half :]
        hid[ty, q] = (g / (1.0 + jnp.exp(-g)) * u).astype(BF16)
        for dy in (2, 1, 3):
            share_out(hid, ty, q, hid_send, hid_recv.at[q], along(dy))

    def stage_f(q):
        if q == 0:
            load_down.wait()
            arrived(wd.at[pl.ds(0, NT - 1)], wd_recv)
        arrived(hid.at[pl.ds(0, NY - 1), q], hid_recv.at[q])
        x = jnp.concatenate([hid[y, q] for y in range(NY)], axis=-1)
        result = jnp.dot(x, wd[...].reshape(NT * half, quarter), preferred_element_type=F32)
        top = jnp.maximum(jnp.max(jnp.abs(result), axis=-1, keepdims=True), 1e-30)
        key = jnp.ceil(jnp.log2(top) * KEYS) + 1.0
        level = jnp.round(result * (LEVELS * jnp.exp2(key * (-1.0 / KEYS)))).astype(jnp.int32)
        for c in range(NC):
            left = level[:, c * share : c * share + 128]
            right = level[:, c * share + 128 : (c + 1) * share]
            outb[q, :, c, 0:cap, :] = ((left << 16) | (right & 0xFFFF)).reshape(PER, cap, 128)
        row = lax.broadcasted_iota(jnp.int32, (work_rows, 128), 0) % cap
        col = lax.broadcasted_iota(jnp.int32, (work_rows, 128), 1)
        keys = jnp.where(col == row + tc * cap + ep % (128 // block) * block, key, 0.0)
        keys = jnp.sum(keys.reshape(PER, cap, 128), axis=1, keepdims=True).astype(jnp.int32)
        for c in range(NC):
            outb[q, :, c, cap : cap + 1, :] = keys

        @pl.when(own_q == q)
        def _():
            r = own_line % LINES * NX + ex
            ret[ep * NC + tc] = outb[q, r, tc]

        for k in range(LINES):
            line = q * LINES + k
            z = ZORDER[line] if ABSOLUTE else (ez + ORDER[line]) % NZ

            @pl.loop(0, NX)
            def _(x):
                e, r = z * NX + x, k * NX + x
                for c in range(NC):

                    @pl.when((e != ep) | (c != tc))
                    def _():
                        t = ty * NC + c
                        send(outb.at[q, r, c], ret.at[ep * NC + tc], ret_send, ret_recv, e, t)

    stages = {"a": stage_a, "b": stage_b, "d": stage_d, "f": stage_f}
    for word in SEQ:
        with jax.named_scope(f"stage_{word}"):
            stages[word[0]](int(word[1:]))

    with jax.named_scope("ret_wait"):
        arrived(ret.at[pl.ds(0, NE * NC - 1)], ret_recv)
    per = 128 // block
    words = ret[:, 0:cap, :].reshape(NE * block, 128)
    back = jnp.concatenate([words >> 16, (words << 16) >> 16], axis=-1).astype(F32)
    keys = ret[:, cap : cap + 1, :].astype(F32)
    keys = jnp.concatenate(
        [jnp.sum(keys[i * per * NC : (i + 1) * per * NC], axis=0) for i in range(NE // per)], axis=-1
    )
    scale = jnp.exp2(keys * (1.0 / KEYS)) * (1.0 / LEVELS)
    out_v[...] = jnp.dot(
        combine[...] * scale, back, preferred_element_type=F32, precision=lax.Precision.HIGHEST
    ).astype(out_v.dtype)

    with jax.named_scope("drain"):
        arrived(packed.at[pl.ds(0, (NE - 1) * block)], disp_send)
        arrived(wd.at[pl.ds(0, NT - 1)], wd_send)
        arrived(wall.at[0], wall_send)
        arrived(gath.at[pl.ds(0, NY - 1)], ag_send)
        arrived(hid.at[pl.ds(0, NY - 1)], hid_send)
        arrived(ret.at[pl.ds(0, NE * NC - 1)], ret_send)


def per_device(tokens, norm_gain, norm_shift, expert_ids, gate_weights, expert_gate, expert_up, expert_down):
    rows, features = tokens.shape
    local, _, half = expert_gate.shape
    quarter = features // NY
    share = features // NT
    cap = rows // 2 * expert_ids.shape[1] // (local * NE // GROUPS)
    block = local * cap
    any_spec = pl.BlockSpec(memory_space=pl.ANY)
    vmem = pl.BlockSpec(memory_space=pltpu.VMEM)
    dma = pltpu.SemaphoreType.DMA
    out = pl.pallas_call(
        kernel,
        out_shape=pltpu.VMEM((rows, share), F32),
        in_specs=[any_spec, vmem, vmem, vmem, vmem, any_spec, any_spec, any_spec],
        out_specs=vmem,
        scratch_shapes=[
            pltpu.VMEM((rows, features), BF16),
            pltpu.VMEM((2, NC, half, features), BF16),
            pltpu.VMEM((NE * block, share), BF16),
            pltpu.VMEM((NY, CHUNKS, PER * block, share), BF16),
            pltpu.VMEM((NT, half, quarter), BF16),
            pltpu.VMEM((NY, CHUNKS, PER * cap, NC * half), BF16),
            pltpu.VMEM((CHUNKS, PER, NC, cap + 1, 128), jnp.int32),
            pltpu.VMEM((NE * NC, cap + 1, 128), jnp.int32),
            pltpu.VMEM((rows, NE * block), F32),
            dma((4,)),
            dma,
            dma((CHUNKS,)),
            dma,
            dma((NY, CHUNKS)),
            dma,
            dma,
            dma,
            dma,
            dma,
            dma((CHUNKS,)),
            dma,
            dma,
        ],
        compiler_params=pltpu.CompilerParams(collective_id=0, has_side_effects=True, vmem_limit_bytes=VMEM_LIMIT),
    )(
        tokens,
        norm_gain.reshape(1, features),
        norm_shift.reshape(1, features),
        expert_ids.T,
        gate_weights.T,
        expert_gate.transpose(0, 2, 1),
        expert_up.transpose(0, 2, 1),
        expert_down,
    )
    return out.astype(BF16)


def solution(mesh):
    return jax.shard_map(
        per_device,
        mesh=mesh,
        in_specs=(
            P("ep", None),
            P(),
            P(),
            P("ep", None),
            P("ep", None),
            P("ep", None, "tp"),
            P("ep", None, "tp"),
            P("ep", "tp", None),
        ),
        out_specs=P("ep", "tp"),
        check_vma=False,
    )
```

```python
import jax
import jax.numpy as jnp
from jax import lax
from jax.experimental import pallas as pl
from jax.experimental.pallas import tpu as pltpu
from jax.sharding import PartitionSpec as P

MESH = pl.DeviceIdType.MESH
GROUPS = 4
NZ, NX, NY, NC = 8, 4, 4, 2
NE, NT = NZ * NX, NY * NC
ABSOLUTE = True
ZORDER = (0, 1, 2, 3, 4, 5, 6, 7)
SEND_FAR = True
SIG_FAR = True
ORDER = (0, 7, 1, 6, 2, 5, 3, 4)
CHUNKS = 4
LINES = NZ // CHUNKS
PER = NE // CHUNKS
FAR_AT = 0
SEQ = ("a0", "a1", "a2", "a3", "d0", "d1", "d2", "d3", "f0", "f1", "f2", "f3")
FINAL_CAST = True
VMEM_LIMIT = 56 * 2**20
epsilon = 1e-05
LEVELS = 32760.0
KEYS = 128.0
F32, BF16 = jnp.float32, jnp.bfloat16


def kernel(
    tokens_h, gain_v, shift_v, ids_v, gw_v, gate_h, up_h, down_h, out_v,
    tok, wall, columns, packed, spare, gath, wd, hid, outb, ret, combine,
    load_sem, disp_send, disp_recv, far_send, far_recv, ag_send, ag_recv, wall_send, wall_recv, wd_send, wd_recv, hid_send, hid_recv,
    ret_send, ret_recv,
):
    ep, tp = lax.axis_index("ep"), lax.axis_index("tp")
    ez, ex = ep // NX, ep % NX
    ty, tc = tp // NC, tp % NC
    mate = ty * NC + 1 - tc
    rows, features = tok.shape
    quarter = features // NY
    share = quarter // NC
    block = packed.shape[0] // NE
    cap = block // NC
    half = wall.shape[2]
    chunk_rows = PER * block
    work_rows = PER * cap
    own_line = sum(jnp.where(ez == z, line, 0) for line, z in enumerate(ZORDER)) if ABSOLUTE else ORDER.index(0)
    own_q = own_line // LINES

    def arrived(ref, sem):
        pltpu.make_async_copy(ref, ref, sem).wait()

    def send(src, dst, send_sem, recv_sem, e, t):
        pltpu.make_async_remote_copy(
            src_ref=src, dst_ref=dst, send_sem=send_sem, recv_sem=recv_sem, device_id=(e, t), device_id_type=MESH
        ).start()

    def rows_of(n):
        return pl.ds(pl.multiple_of(n * block, block), block)

    def quarter_of(y):
        return pl.ds(pl.multiple_of(y * quarter, quarter), quarter)

    load_tok = pltpu.make_async_copy(tokens_h, tok, load_sem.at[0])
    load_gate = pltpu.make_async_copy(gate_h.at[tc], wall.at[0, tc], load_sem.at[1])
    load_up = pltpu.make_async_copy(up_h.at[tc], wall.at[1, tc], load_sem.at[2])
    load_down = pltpu.make_async_copy(down_h.at[tc, :, quarter_of(ty)], wd.at[tp], load_sem.at[3])
    load_tok.start()

    barrier = pltpu.get_barrier_semaphore()

    def signal(e, t):
        pl.semaphore_signal(barrier, inc=1, device_id=(e, t), device_id_type=MESH)

    for dz in (4, 3, 5, 2, 6, 1, 7, 0):
        for dx in range(1 if dz == 0 else 0, NX):
            signal(((ez + dz) % NZ) * NX + (ex + dx) % NX, tp)
    for d in range(1, NT):
        signal(ep, (tp + d) % NT)

    ids, gw = ids_v[...], gw_v[...]
    earlier = lax.broadcasted_iota(jnp.int32, (rows, rows), 0) < lax.broadcasted_iota(jnp.int32, (rows, rows), 1)
    earlier = jnp.where(earlier, 1.0, 0.0).astype(BF16)

    def placed(numbers):
        hits = jnp.zeros(numbers.shape, F32)
        weights = jnp.zeros(numbers.shape, F32)
        for k in range(ids.shape[0]):
            same = ids[k : k + 1, :] == numbers
            hits = hits + jnp.where(same, 1.0, 0.0)
            weights = weights + jnp.where(same, gw[k : k + 1, :], 0.0)
        before = jnp.dot(hits.astype(BF16), earlier, preferred_element_type=F32)
        code = hits * (before + 1.0)
        wanted = (lax.broadcasted_iota(jnp.int32, (numbers.shape[0], cap, rows), 1) + 1).astype(F32)
        return code[:, None, :] == wanted, weights

    with jax.named_scope("p_place"):
        place, _ = placed(lax.broadcasted_iota(jnp.int32, (NE, rows), 0) * NC + tc)
        place = jnp.where(place, 1.0, 0.0).reshape(NE * cap, rows).astype(BF16)

    load_tok.wait()
    load_gate.start()
    load_up.start()
    load_down.start()
    with jax.named_scope("p_ln"):
        values = tok[...].astype(F32)
        centre = jnp.mean(values, axis=-1, keepdims=True)
        spread = jnp.mean(jnp.square(values - centre), axis=-1, keepdims=True)
        scale = lax.rsqrt(spread + epsilon)

        def pack(y, buf):
            own = tok[:, quarter_of(y)].astype(F32)
            normed = (own - centre) * scale * gain_v[:, quarter_of(y)] + shift_v[:, quarter_of(y)]
            picked = jnp.dot(place, normed.astype(BF16), preferred_element_type=F32).reshape(NE, cap, quarter)
            picked = jnp.stack([picked[:, :, :share], picked[:, :, share:]], axis=1)
            buf[...] = picked.reshape(NE * block, share).astype(BF16)
            gath[y, own_q, rows_of(own_line % LINES * NX + ex), :] = buf[rows_of(ep), :]

        pack(ty, packed)

    with jax.named_scope("entry_wait"):
        pl.semaphore_wait(barrier, NE - 1 + NT - 1)

    def dispatch(buf, y, send_sem, recv_sem):
        sends = tuple(enumerate(ORDER))
        for line, dz in reversed(sends) if SEND_FAR else sends:
            line = own_line if ABSOLUTE else line

            @pl.loop(1 if dz == 0 else 0, NX)
            def _(dx):
                e = ((ez + NZ - dz) % NZ) * NX + (ex + dx) % NX
                send(
                    buf.at[rows_of(e)], gath.at[y, line // LINES, rows_of(line % LINES * NX + ex)],
                    send_sem, recv_sem.at[line // LINES], e, tp,
                )

    dispatch(packed, ty, disp_send, disp_recv)

    for d in range(1, NT):
        t = (tp + d) % NT
        send(down_h.at[t % NC, :, quarter_of(t // NC)], wd.at[tp], wd_send, wd_recv, ep, t)

    send(gate_h.at[1 - tc], wall.at[0, tc], wall_send, wall_recv, ep, mate)
    send(up_h.at[1 - tc], wall.at[1, tc], wall_send, wall_recv, ep, mate)

    far = (ty + 2) % NY
    if FAR_AT == 0:
        pack(far, spare)
        dispatch(spare, far, far_send, far_recv)

    with jax.named_scope("p_combine"):
        place, weights = placed(lax.broadcasted_iota(jnp.int32, (NE * NC, rows), 0))
        w_slots = jnp.where(place, weights[:, None, :], 0.0).reshape(NE * block, rows)
        combine[...] = w_slots.T

    with jax.named_scope("p_columns"):
        load_gate.wait()
        load_up.wait()
        arrived(wall.at[0], wall_recv)
        for i in range(0, features, quarter):
            columns[i : i + quarter, :] = wall[:, :, :, i : i + quarter].reshape(2 * NC * half, quarter).T

    if FAR_AT == 1:
        pack(far, spare)
        dispatch(spare, far, far_send, far_recv)

    def share_out(buf, y, q, send_sem, recv_sem, to, part=None):
        ref = buf.at[y, q] if part is None else buf.at[y, q, part]
        send(ref, ref, send_sem, recv_sem, ep, to * NC + tc)

    def along(dy):
        return (ty + dy) % NY

    def from_sources(y, q, recv_sem):
        @pl.when(own_q == q)
        def _():
            arrived(gath.at[y, q, pl.ds(0, chunk_rows - block)], recv_sem.at[q])

        @pl.when(own_q != q)
        def _():
            arrived(gath.at[y, q], recv_sem.at[q])

    def stage_a(q):
        from_sources(ty, q, disp_recv)
        share_out(gath, ty, q, ag_send, ag_recv.at[ty, q], along(1))
        share_out(gath, ty, q, ag_send, ag_recv.at[ty, q], along(3))

    def stage_d(q):
        from_sources(far, q, far_recv)
        for dy in (1, 3):
            arrived(gath.at[along(dy), q], ag_recv.at[along(dy), q])
        parts = []
        for y in range(NY):
            both = gath[y, q].astype(F32).reshape(PER, NC, cap, share)
            parts += [both[:, i].reshape(work_rows, share).astype(BF16) for i in range(NC)]
        x = jnp.concatenate(parts, axis=-1)
        both = jnp.dot(x, columns[...], preferred_element_type=F32)
        g, u = both[:, : NC * half], both[:, NC * half :]
        hid[ty, q] = (g / (1.0 + jnp.exp(-g)) * u).astype(BF16)
        for dy in (2, 1, 3):
            share_out(hid, ty, q, hid_send, hid_recv.at[q], along(dy))

    def stage_f(q):
        if q == 0:
            load_down.wait()
            arrived(wd.at[pl.ds(0, NT - 1)], wd_recv)
        arrived(hid.at[pl.ds(0, NY - 1), q], hid_recv.at[q])
        x = jnp.concatenate([hid[y, q] for y in range(NY)], axis=-1)
        result = jnp.dot(x, wd[...].reshape(NT * half, quarter), preferred_element_type=F32)
        top = jnp.maximum(jnp.max(jnp.abs(result), axis=-1, keepdims=True), 1e-30)
        key = jnp.ceil(jnp.log2(top) * KEYS) + 1.0
        level = jnp.round(result * (LEVELS * jnp.exp2(key * (-1.0 / KEYS)))).astype(jnp.int32)
        for c in range(NC):
            left = level[:, c * share : c * share + 128]
            right = level[:, c * share + 128 : (c + 1) * share]
            outb[q, :, c, 0:cap, :] = ((left << 16) | (right & 0xFFFF)).reshape(PER, cap, 128)
        row = lax.broadcasted_iota(jnp.int32, (work_rows, 128), 0) % cap
        col = lax.broadcasted_iota(jnp.int32, (work_rows, 128), 1)
        keys = jnp.where(col == row + tc * cap + ep % (128 // block) * block, key, 0.0)
        keys = jnp.sum(keys.reshape(PER, cap, 128), axis=1, keepdims=True).astype(jnp.int32)
        for c in range(NC):
            outb[q, :, c, cap : cap + 1, :] = keys

        @pl.when(own_q == q)
        def _():
            r = own_line % LINES * NX + ex
            ret[ep * NC + tc] = outb[q, r, tc]

        for k in range(LINES):
            line = q * LINES + k
            z = ZORDER[line] if ABSOLUTE else (ez + ORDER[line]) % NZ

            @pl.loop(0, NX)
            def _(x):
                e, r = z * NX + x, k * NX + x
                for c in range(NC):

                    @pl.when((e != ep) | (c != tc))
                    def _():
                        t = ty * NC + c
                        send(outb.at[q, r, c], ret.at[ep * NC + tc], ret_send, ret_recv, e, t)

    stages = {"a": stage_a, "d": stage_d, "f": stage_f}
    for word in SEQ:
        with jax.named_scope(f"stage_{word}"):
            stages[word[0]](int(word[1:]))

    with jax.named_scope("ret_wait"):
        arrived(ret.at[pl.ds(0, NE * NC - 1)], ret_recv)
    per = 128 // block
    words = ret[:, 0:cap, :].reshape(NE * block, 128)
    back = jnp.concatenate([words >> 16, (words << 16) >> 16], axis=-1).astype(F32)
    keys = ret[:, cap : cap + 1, :].astype(F32)
    keys = jnp.concatenate(
        [jnp.sum(keys[i * per * NC : (i + 1) * per * NC], axis=0) for i in range(NE // per)], axis=-1
    )
    scale = jnp.exp2(keys * (1.0 / KEYS)) * (1.0 / LEVELS)
    out_v[...] = jnp.dot(
        combine[...] * scale, back, preferred_element_type=F32, precision=lax.Precision.HIGHEST
    ).astype(out_v.dtype)

    with jax.named_scope("drain"):
        arrived(packed.at[pl.ds(0, (NE - 1) * block)], disp_send)
        arrived(wd.at[pl.ds(0, NT - 1)], wd_send)
        arrived(wall.at[0], wall_send)
        arrived(gath.at[pl.ds(0, 2)], ag_send)
        arrived(packed.at[pl.ds(0, (NE - 1) * block)], far_send)
        arrived(hid.at[pl.ds(0, NY - 1)], hid_send)
        arrived(ret.at[pl.ds(0, NE * NC - 1)], ret_send)


def per_device(tokens, norm_gain, norm_shift, expert_ids, gate_weights, expert_gate, expert_up, expert_down):
    rows, features = tokens.shape
    local, _, half = expert_gate.shape
    quarter = features // NY
    share = features // NT
    cap = rows // 2 * expert_ids.shape[1] // (local * NE // GROUPS)
    block = local * cap
    any_spec = pl.BlockSpec(memory_space=pl.ANY)
    vmem = pl.BlockSpec(memory_space=pltpu.VMEM)
    dma = pltpu.SemaphoreType.DMA
    out = pl.pallas_call(
        kernel,
        out_shape=pltpu.VMEM((rows, share), F32),
        in_specs=[any_spec, vmem, vmem, vmem, vmem, any_spec, any_spec, any_spec],
        out_specs=vmem,
        scratch_shapes=[
            pltpu.VMEM((rows, features), BF16),
            pltpu.VMEM((2, NC, half, features), BF16),
            pltpu.VMEM((features, 2 * NC * half), BF16),
            pltpu.VMEM((NE * block, share), BF16),
            pltpu.VMEM((NE * block, share), BF16),
            pltpu.VMEM((NY, CHUNKS, PER * block, share), BF16),
            pltpu.VMEM((NT, half, quarter), BF16),
            pltpu.VMEM((NY, CHUNKS, PER * cap, NC * half), BF16),
            pltpu.VMEM((CHUNKS, PER, NC, cap + 1, 128), jnp.int32),
            pltpu.VMEM((NE * NC, cap + 1, 128), jnp.int32),
            pltpu.VMEM((rows, NE * block), F32),
            dma((4,)),
            dma,
            dma((CHUNKS,)),
            dma,
            dma((CHUNKS,)),
            dma,
            dma((NY, CHUNKS)),
            dma,
            dma,
            dma,
            dma,
            dma,
            dma((CHUNKS,)),
            dma,
            dma,
        ],
        compiler_params=pltpu.CompilerParams(collective_id=0, has_side_effects=True, vmem_limit_bytes=VMEM_LIMIT),
    )(
        tokens,
        norm_gain.reshape(1, features),
        norm_shift.reshape(1, features),
        expert_ids.T,
        gate_weights.T,
        expert_gate.transpose(0, 2, 1),
        expert_up.transpose(0, 2, 1),
        expert_down,
    )
    return out.astype(BF16)


def solution(mesh):
    return jax.shard_map(
        per_device,
        mesh=mesh,
        in_specs=(
            P("ep", None),
            P(),
            P(),
            P("ep", None),
            P("ep", None),
            P("ep", None, "tp"),
            P("ep", None, "tp"),
            P("ep", "tp", None),
        ),
        out_specs=P("ep", "tp"),
        check_vma=False,
    )
```

```python
import jax
import jax.numpy as jnp
from jax import lax
from jax.experimental import pallas as pl
from jax.experimental.pallas import tpu as pltpu
from jax.sharding import PartitionSpec as P

MESH = pl.DeviceIdType.MESH
GROUPS = 4
NZ, NX, NY, NC = 8, 4, 4, 2
NE, NT = NZ * NX, NY * NC
ABSOLUTE = True
ZORDER = (0, 1, 2, 3, 4, 5, 6, 7)
SEND_FAR = True
SIG_FAR = True
ORDER = (0, 7, 1, 6, 2, 5, 3, 4)
CHUNKS = 4
LINES = NZ // CHUNKS
PER = NE // CHUNKS
FAR_AT = 1
WD_AT = 0
FAR_FAR = True
SEQ = ("a0", "a1", "a2", "a3", "d0", "d1", "d2", "d3", "f0", "f1", "f2", "f3")
FINAL_CAST = True
VMEM_LIMIT = 56 * 2**20
epsilon = 1e-05
LEVELS = 32760.0
KEYS = 128.0
F32, BF16 = jnp.float32, jnp.bfloat16


def kernel(
    tokens_h, gain_v, shift_v, ids_v, gw_v, gate_h, up_h, down_h, out_v,
    tok, wall, columns, packed, spare, gath, wd, hid, outb, ret, combine,
    load_sem, disp_send, disp_recv, far_send, far_recv, ag_send, ag_recv, wall_send, wall_recv, wd_send, wd_recv, hid_send, hid_recv,
    ret_send, ret_recv,
):
    ep, tp = lax.axis_index("ep"), lax.axis_index("tp")
    ez, ex = ep // NX, ep % NX
    ty, tc = tp // NC, tp % NC
    mate = ty * NC + 1 - tc
    rows, features = tok.shape
    quarter = features // NY
    share = quarter // NC
    block = packed.shape[0] // NE
    cap = block // NC
    half = wall.shape[2]
    chunk_rows = PER * block
    work_rows = PER * cap
    own_line = sum(jnp.where(ez == z, line, 0) for line, z in enumerate(ZORDER)) if ABSOLUTE else ORDER.index(0)
    own_q = own_line // LINES

    def arrived(ref, sem):
        pltpu.make_async_copy(ref, ref, sem).wait()

    def send(src, dst, send_sem, recv_sem, e, t):
        pltpu.make_async_remote_copy(
            src_ref=src, dst_ref=dst, send_sem=send_sem, recv_sem=recv_sem, device_id=(e, t), device_id_type=MESH
        ).start()

    def rows_of(n):
        return pl.ds(pl.multiple_of(n * block, block), block)

    def quarter_of(y):
        return pl.ds(pl.multiple_of(y * quarter, quarter), quarter)

    load_tok = pltpu.make_async_copy(tokens_h, tok, load_sem.at[0])
    load_gate = pltpu.make_async_copy(gate_h.at[tc], wall.at[0, tc], load_sem.at[1])
    load_up = pltpu.make_async_copy(up_h.at[tc], wall.at[1, tc], load_sem.at[2])
    load_down = pltpu.make_async_copy(down_h.at[tc, :, quarter_of(ty)], wd.at[tp], load_sem.at[3])
    load_tok.start()

    barrier = pltpu.get_barrier_semaphore()

    def signal(e, t):
        pl.semaphore_signal(barrier, inc=1, device_id=(e, t), device_id_type=MESH)

    for dz in (4, 3, 5, 2, 6, 1, 7, 0):
        for dx in range(1 if dz == 0 else 0, NX):
            signal(((ez + dz) % NZ) * NX + (ex + dx) % NX, tp)
    for d in range(1, NT):
        signal(ep, (tp + d) % NT)

    ids, gw = ids_v[...], gw_v[...]
    earlier = lax.broadcasted_iota(jnp.int32, (rows, rows), 0) < lax.broadcasted_iota(jnp.int32, (rows, rows), 1)
    earlier = jnp.where(earlier, 1.0, 0.0).astype(BF16)

    def placed(numbers):
        hits = jnp.zeros(numbers.shape, F32)
        weights = jnp.zeros(numbers.shape, F32)
        for k in range(ids.shape[0]):
            same = ids[k : k + 1, :] == numbers
            hits = hits + jnp.where(same, 1.0, 0.0)
            weights = weights + jnp.where(same, gw[k : k + 1, :], 0.0)
        before = jnp.dot(hits.astype(BF16), earlier, preferred_element_type=F32)
        code = hits * (before + 1.0)
        wanted = (lax.broadcasted_iota(jnp.int32, (numbers.shape[0], cap, rows), 1) + 1).astype(F32)
        return code[:, None, :] == wanted, weights

    with jax.named_scope("p_place"):
        place, _ = placed(lax.broadcasted_iota(jnp.int32, (NE, rows), 0) * NC + tc)
        place = jnp.where(place, 1.0, 0.0).reshape(NE * cap, rows).astype(BF16)

    load_tok.wait()
    load_gate.start()
    load_up.start()
    load_down.start()
    with jax.named_scope("p_ln"):
        values = tok[...].astype(F32)
        centre = jnp.mean(values, axis=-1, keepdims=True)
        spread = jnp.mean(jnp.square(values - centre), axis=-1, keepdims=True)
        scale = lax.rsqrt(spread + epsilon)

        def pack(y, buf):
            own = tok[:, quarter_of(y)].astype(F32)
            normed = (own - centre) * scale * gain_v[:, quarter_of(y)] + shift_v[:, quarter_of(y)]
            picked = jnp.dot(place, normed.astype(BF16), preferred_element_type=F32).reshape(NE, cap, quarter)
            picked = jnp.stack([picked[:, :, :share], picked[:, :, share:]], axis=1)
            buf[...] = picked.reshape(NE * block, share).astype(BF16)
            gath[y, own_q, rows_of(own_line % LINES * NX + ex), :] = buf[rows_of(ep), :]

        pack(ty, packed)

    with jax.named_scope("entry_wait"):
        pl.semaphore_wait(barrier, NE - 1 + NT - 1)

    def dispatch(buf, y, send_sem, recv_sem, farthest=SEND_FAR):
        sends = tuple(enumerate(ORDER))
        for line, dz in reversed(sends) if farthest else sends:
            line = own_line if ABSOLUTE else line

            @pl.loop(1 if dz == 0 else 0, NX)
            def _(dx):
                e = ((ez + NZ - dz) % NZ) * NX + (ex + dx) % NX
                send(
                    buf.at[rows_of(e)], gath.at[y, line // LINES, rows_of(line % LINES * NX + ex)],
                    send_sem, recv_sem.at[line // LINES], e, tp,
                )

    dispatch(packed, ty, disp_send, disp_recv)

    def exchange_down():
        for d in range(1, NT):
            t = (tp + d) % NT
            send(down_h.at[t % NC, :, quarter_of(t // NC)], wd.at[tp], wd_send, wd_recv, ep, t)

    if WD_AT == 0:
        exchange_down()

    send(gate_h.at[1 - tc], wall.at[0, tc], wall_send, wall_recv, ep, mate)
    send(up_h.at[1 - tc], wall.at[1, tc], wall_send, wall_recv, ep, mate)

    far = (ty + 2) % NY
    if FAR_AT == 0:
        pack(far, spare)
        dispatch(spare, far, far_send, far_recv, FAR_FAR)

    with jax.named_scope("p_combine"):
        every, weights = placed(lax.broadcasted_iota(jnp.int32, (NE * NC, rows), 0))
        w_slots = jnp.where(every, weights[:, None, :], 0.0).reshape(NE * block, rows)
        combine[...] = w_slots.T

    if WD_AT == 1:
        exchange_down()
    if FAR_AT == 2:
        pack(far, spare)
        dispatch(spare, far, far_send, far_recv, FAR_FAR)

    with jax.named_scope("p_columns"):
        load_gate.wait()
        load_up.wait()
        arrived(wall.at[0], wall_recv)
        for i in range(0, features, quarter):
            columns[i : i + quarter, :] = wall[:, :, :, i : i + quarter].reshape(2 * NC * half, quarter).T

    if FAR_AT == 1:
        pack(far, spare)
        dispatch(spare, far, far_send, far_recv, FAR_FAR)

    def share_out(buf, y, q, send_sem, recv_sem, to, part=None):
        ref = buf.at[y, q] if part is None else buf.at[y, q, part]
        send(ref, ref, send_sem, recv_sem, ep, to * NC + tc)

    def along(dy):
        return (ty + dy) % NY

    def from_sources(y, q, recv_sem):
        @pl.when(own_q == q)
        def _():
            arrived(gath.at[y, q, pl.ds(0, chunk_rows - block)], recv_sem.at[q])

        @pl.when(own_q != q)
        def _():
            arrived(gath.at[y, q], recv_sem.at[q])

    def stage_a(q):
        from_sources(ty, q, disp_recv)
        share_out(gath, ty, q, ag_send, ag_recv.at[ty, q], along(1))
        share_out(gath, ty, q, ag_send, ag_recv.at[ty, q], along(3))

    def stage_d(q):
        from_sources(far, q, far_recv)
        for dy in (1, 3):
            arrived(gath.at[along(dy), q], ag_recv.at[along(dy), q])
        parts = []
        for y in range(NY):
            both = gath[y, q].astype(F32).reshape(PER, NC, cap, share)
            parts += [both[:, i].reshape(work_rows, share).astype(BF16) for i in range(NC)]
        x = jnp.concatenate(parts, axis=-1)
        both = jnp.dot(x, columns[...], preferred_element_type=F32)
        g, u = both[:, : NC * half], both[:, NC * half :]
        hid[ty, q] = (g / (1.0 + jnp.exp(-g)) * u).astype(BF16)
        for dy in (2, 1, 3):
            share_out(hid, ty, q, hid_send, hid_recv.at[q], along(dy))

    def stage_f(q):
        if q == 0:
            load_down.wait()
            arrived(wd.at[pl.ds(0, NT - 1)], wd_recv)
        arrived(hid.at[pl.ds(0, NY - 1), q], hid_recv.at[q])
        x = jnp.concatenate([hid[y, q] for y in range(NY)], axis=-1)
        result = jnp.dot(x, wd[...].reshape(NT * half, quarter), preferred_element_type=F32)
        top = jnp.maximum(jnp.max(jnp.abs(result), axis=-1, keepdims=True), 1e-30)
        key = jnp.ceil(jnp.log2(top) * KEYS) + 1.0
        level = jnp.round(result * (LEVELS * jnp.exp2(key * (-1.0 / KEYS)))).astype(jnp.int32)
        for c in range(NC):
            left = level[:, c * share : c * share + 128]
            right = level[:, c * share + 128 : (c + 1) * share]
            outb[q, :, c, 0:cap, :] = ((left << 16) | (right & 0xFFFF)).reshape(PER, cap, 128)
        row = lax.broadcasted_iota(jnp.int32, (work_rows, 128), 0) % cap
        col = lax.broadcasted_iota(jnp.int32, (work_rows, 128), 1)
        keys = jnp.where(col == row + tc * cap + ep % (128 // block) * block, key, 0.0)
        keys = jnp.sum(keys.reshape(PER, cap, 128), axis=1, keepdims=True).astype(jnp.int32)
        for c in range(NC):
            outb[q, :, c, cap : cap + 1, :] = keys

        @pl.when(own_q == q)
        def _():
            r = own_line % LINES * NX + ex
            ret[ep * NC + tc] = outb[q, r, tc]

        for k in range(LINES):
            line = q * LINES + k
            z = ZORDER[line] if ABSOLUTE else (ez + ORDER[line]) % NZ

            @pl.loop(0, NX)
            def _(x):
                e, r = z * NX + x, k * NX + x
                for c in range(NC):

                    @pl.when((e != ep) | (c != tc))
                    def _():
                        t = ty * NC + c
                        send(outb.at[q, r, c], ret.at[ep * NC + tc], ret_send, ret_recv, e, t)

    stages = {"a": stage_a, "d": stage_d, "f": stage_f}
    for word in SEQ:
        with jax.named_scope(f"stage_{word}"):
            stages[word[0]](int(word[1:]))

    with jax.named_scope("ret_wait"):
        arrived(ret.at[pl.ds(0, NE * NC - 1)], ret_recv)
    per = 128 // block
    words = ret[:, 0:cap, :].reshape(NE * block, 128)
    back = jnp.concatenate([words >> 16, (words << 16) >> 16], axis=-1).astype(F32)
    keys = ret[:, cap : cap + 1, :].astype(F32)
    keys = jnp.concatenate(
        [jnp.sum(keys[i * per * NC : (i + 1) * per * NC], axis=0) for i in range(NE // per)], axis=-1
    )
    scale = jnp.exp2(keys * (1.0 / KEYS)) * (1.0 / LEVELS)
    out_v[...] = jnp.dot(
        combine[...] * scale, back, preferred_element_type=F32, precision=lax.Precision.HIGHEST
    ).astype(out_v.dtype)

    with jax.named_scope("drain"):
        arrived(packed.at[pl.ds(0, (NE - 1) * block)], disp_send)
        arrived(wd.at[pl.ds(0, NT - 1)], wd_send)
        arrived(wall.at[0], wall_send)
        arrived(gath.at[pl.ds(0, 2)], ag_send)
        arrived(packed.at[pl.ds(0, (NE - 1) * block)], far_send)
        arrived(hid.at[pl.ds(0, NY - 1)], hid_send)
        arrived(ret.at[pl.ds(0, NE * NC - 1)], ret_send)


def per_device(tokens, norm_gain, norm_shift, expert_ids, gate_weights, expert_gate, expert_up, expert_down):
    rows, features = tokens.shape
    local, _, half = expert_gate.shape
    quarter = features // NY
    share = features // NT
    cap = rows // 2 * expert_ids.shape[1] // (local * NE // GROUPS)
    block = local * cap
    any_spec = pl.BlockSpec(memory_space=pl.ANY)
    vmem = pl.BlockSpec(memory_space=pltpu.VMEM)
    dma = pltpu.SemaphoreType.DMA
    out = pl.pallas_call(
        kernel,
        out_shape=pltpu.VMEM((rows, share), F32),
        in_specs=[any_spec, vmem, vmem, vmem, vmem, any_spec, any_spec, any_spec],
        out_specs=vmem,
        scratch_shapes=[
            pltpu.VMEM((rows, features), BF16),
            pltpu.VMEM((2, NC, half, features), BF16),
            pltpu.VMEM((features, 2 * NC * half), BF16),
            pltpu.VMEM((NE * block, share), BF16),
            pltpu.VMEM((NE * block, share), BF16),
            pltpu.VMEM((NY, CHUNKS, PER * block, share), BF16),
            pltpu.VMEM((NT, half, quarter), BF16),
            pltpu.VMEM((NY, CHUNKS, PER * cap, NC * half), BF16),
            pltpu.VMEM((CHUNKS, PER, NC, cap + 1, 128), jnp.int32),
            pltpu.VMEM((NE * NC, cap + 1, 128), jnp.int32),
            pltpu.VMEM((rows, NE * block), F32),
            dma((4,)),
            dma,
            dma((CHUNKS,)),
            dma,
            dma((CHUNKS,)),
            dma,
            dma((NY, CHUNKS)),
            dma,
            dma,
            dma,
            dma,
            dma,
            dma((CHUNKS,)),
            dma,
            dma,
        ],
        compiler_params=pltpu.CompilerParams(collective_id=0, has_side_effects=True, vmem_limit_bytes=VMEM_LIMIT),
    )(
        tokens,
        norm_gain.reshape(1, features),
        norm_shift.reshape(1, features),
        expert_ids.T,
        gate_weights.T,
        expert_gate.transpose(0, 2, 1),
        expert_up.transpose(0, 2, 1),
        expert_down,
    )
    return out.astype(BF16)


def solution(mesh):
    return jax.shard_map(
        per_device,
        mesh=mesh,
        in_specs=(
            P("ep", None),
            P(),
            P(),
            P("ep", None),
            P("ep", None),
            P("ep", None, "tp"),
            P("ep", None, "tp"),
            P("ep", "tp", None),
        ),
        out_specs=P("ep", "tp"),
        check_vma=False,
    )
```

```python
import jax
import jax.numpy as jnp
from jax import lax
from jax.experimental import pallas as pl
from jax.experimental.pallas import tpu as pltpu
from jax.sharding import PartitionSpec as P

MESH = pl.DeviceIdType.MESH
GROUPS = 4
NZ, NX, NY, NC = 8, 4, 4, 2
NE, NT = NZ * NX, NY * NC
ABSOLUTE = True
ZORDER = (0, 4, 1, 5, 2, 6, 3, 7)
SEND_FAR = True
SIG_FAR = True
ORDER = (0, 7, 1, 6, 2, 5, 3, 4)
CHUNKS = 4
LINES = NZ // CHUNKS
PER = NE // CHUNKS
FAR_AT = 1
WD_AT = 0
FAR_FAR = True
SEQ = ("a0", "a1", "a2", "a3", "d0", "d1", "d2", "d3", "f0", "f1", "f2", "f3")
FINAL_CAST = True
VMEM_LIMIT = 56 * 2**20
epsilon = 1e-05
LEVELS = 32760.0
KEYS = 128.0
F32, BF16 = jnp.float32, jnp.bfloat16


def weighted(weights, codes):
    high = (codes + 128) >> 8
    low = codes - (high << 8)
    parts, rest = [], weights
    for _ in range(3):
        parts.append(rest.astype(BF16))
        rest = rest - parts[-1].astype(F32)
    left = jnp.concatenate(parts, axis=0)
    right = jnp.concatenate([high.astype(F32).astype(BF16), low.astype(F32).astype(BF16)], axis=-1)
    terms = jnp.dot(left, right, preferred_element_type=F32)
    n, m = weights.shape[0], codes.shape[1]
    terms = terms[:n] + terms[n : 2 * n] + terms[2 * n :]
    return terms[:, :m] * 256.0 + terms[:, m:]


def kernel(
    tokens_h, gain_v, shift_v, ids_v, gw_v, gate_h, up_h, down_h, out_v,
    tok, wall, columns, packed, spare, gath, wd, hid, outb, ret, combine,
    load_sem, disp_send, disp_recv, far_send, far_recv, ag_send, ag_recv, wall_send, wall_recv, wd_send, wd_recv, hid_send, hid_recv,
    ret_send, ret_recv,
):
    ep, tp = lax.axis_index("ep"), lax.axis_index("tp")
    ez, ex = ep // NX, ep % NX
    ty, tc = tp // NC, tp % NC
    mate = ty * NC + 1 - tc
    rows, features = tok.shape
    quarter = features // NY
    share = quarter // NC
    block = packed.shape[0] // NE
    cap = block // NC
    half = wall.shape[2]
    chunk_rows = PER * block
    work_rows = PER * cap
    own_line = sum(jnp.where(ez == z, line, 0) for line, z in enumerate(ZORDER)) if ABSOLUTE else ORDER.index(0)
    own_q = own_line // LINES

    def arrived(ref, sem):
        pltpu.make_async_copy(ref, ref, sem).wait()

    def send(src, dst, send_sem, recv_sem, e, t):
        pltpu.make_async_remote_copy(
            src_ref=src, dst_ref=dst, send_sem=send_sem, recv_sem=recv_sem, device_id=(e, t), device_id_type=MESH
        ).start()

    def rows_of(n):
        return pl.ds(pl.multiple_of(n * block, block), block)

    def quarter_of(y):
        return pl.ds(pl.multiple_of(y * quarter, quarter), quarter)

    load_tok = pltpu.make_async_copy(tokens_h, tok, load_sem.at[0])
    load_gate = pltpu.make_async_copy(gate_h.at[tc], wall.at[0, tc], load_sem.at[1])
    load_up = pltpu.make_async_copy(up_h.at[tc], wall.at[1, tc], load_sem.at[2])
    load_down = pltpu.make_async_copy(down_h.at[tc, :, quarter_of(ty)], wd.at[tp], load_sem.at[3])
    load_tok.start()

    barrier = pltpu.get_barrier_semaphore()

    def signal(e, t):
        pl.semaphore_signal(barrier, inc=1, device_id=(e, t), device_id_type=MESH)

    for dz in (0, 1, 7, 2, 6, 3, 5, 4):
        for dx in range(1 if dz == 0 else 0, NX):
            signal(((ez + dz) % NZ) * NX + (ex + dx) % NX, tp)
    for d in range(1, NT):
        signal(ep, (tp + d) % NT)

    ids, gw = ids_v[...], gw_v[...]
    earlier = lax.broadcasted_iota(jnp.int32, (rows, rows), 0) < lax.broadcasted_iota(jnp.int32, (rows, rows), 1)
    earlier = jnp.where(earlier, 1.0, 0.0).astype(BF16)

    def placed(numbers):
        hits = jnp.zeros(numbers.shape, F32)
        weights = jnp.zeros(numbers.shape, F32)
        for k in range(ids.shape[0]):
            same = ids[k : k + 1, :] == numbers
            hits = hits + jnp.where(same, 1.0, 0.0)
            weights = weights + jnp.where(same, gw[k : k + 1, :], 0.0)
        before = jnp.dot(hits.astype(BF16), earlier, preferred_element_type=F32)
        code = hits * (before + 1.0)
        wanted = (lax.broadcasted_iota(jnp.int32, (numbers.shape[0], cap, rows), 1) + 1).astype(F32)
        return code[:, None, :] == wanted, weights

    with jax.named_scope("p_place"):
        place, _ = placed(lax.broadcasted_iota(jnp.int32, (NE, rows), 0) * NC + tc)
        place = jnp.where(place, 1.0, 0.0).reshape(NE * cap, rows).astype(BF16)

    load_tok.wait()
    load_gate.start()
    load_up.start()
    load_down.start()
    with jax.named_scope("p_ln"):
        values = tok[...].astype(F32)
        centre = jnp.mean(values, axis=-1, keepdims=True)
        spread = jnp.mean(jnp.square(values - centre), axis=-1, keepdims=True)
        scale = lax.rsqrt(spread + epsilon)

        def pack(y, buf):
            own = tok[:, quarter_of(y)].astype(F32)
            normed = (own - centre) * scale * gain_v[:, quarter_of(y)] + shift_v[:, quarter_of(y)]
            picked = jnp.dot(place, normed.astype(BF16), preferred_element_type=F32).reshape(NE, cap, quarter)
            picked = jnp.stack([picked[:, :, :share], picked[:, :, share:]], axis=1)
            buf[...] = picked.reshape(NE * block, share).astype(BF16)
            gath[y, own_q, rows_of(own_line % LINES * NX + ex), :] = buf[rows_of(ep), :]

        pack(ty, packed)

    with jax.named_scope("entry_wait"):
        pl.semaphore_wait(barrier, NE - 1 + NT - 1)

    def dispatch(buf, y, send_sem, recv_sem, farthest=SEND_FAR):
        sends = tuple(enumerate(ORDER))
        for line, dz in reversed(sends) if farthest else sends:
            line = own_line if ABSOLUTE else line

            @pl.loop(1 if dz == 0 else 0, NX)
            def _(dx):
                e = ((ez + NZ - dz) % NZ) * NX + (ex + dx) % NX
                send(
                    buf.at[rows_of(e)], gath.at[y, line // LINES, rows_of(line % LINES * NX + ex)],
                    send_sem, recv_sem.at[line // LINES], e, tp,
                )

    dispatch(packed, ty, disp_send, disp_recv)

    def exchange_down():
        for d in range(1, NT):
            t = (tp + d) % NT
            send(down_h.at[t % NC, :, quarter_of(t // NC)], wd.at[tp], wd_send, wd_recv, ep, t)

    if WD_AT == 0:
        exchange_down()

    send(gate_h.at[1 - tc], wall.at[0, tc], wall_send, wall_recv, ep, mate)
    send(up_h.at[1 - tc], wall.at[1, tc], wall_send, wall_recv, ep, mate)

    far = (ty + 2) % NY
    if FAR_AT == 0:
        pack(far, spare)
        dispatch(spare, far, far_send, far_recv, FAR_FAR)

    with jax.named_scope("p_combine"):
        number = lax.broadcasted_iota(jnp.int32, (NE * NC, rows), 0)
        every, weights = placed(number % NE * NC + number // NE)
        w_slots = jnp.where(every, weights[:, None, :], 0.0).reshape(NE * block, rows)
        for c in range(NC):
            combine[c] = w_slots[c * NE * cap : (c + 1) * NE * cap].T

    if WD_AT == 1:
        exchange_down()
    if FAR_AT == 2:
        pack(far, spare)
        dispatch(spare, far, far_send, far_recv, FAR_FAR)

    with jax.named_scope("p_columns"):
        load_gate.wait()
        load_up.wait()
        arrived(wall.at[0], wall_recv)
        for i in range(0, features, quarter):
            columns[i : i + quarter, :] = wall[:, :, :, i : i + quarter].reshape(2 * NC * half, quarter).T

    if FAR_AT == 1:
        pack(far, spare)
        dispatch(spare, far, far_send, far_recv, FAR_FAR)

    def share_out(buf, y, q, send_sem, recv_sem, to, part=None):
        ref = buf.at[y, q] if part is None else buf.at[y, q, part]
        send(ref, ref, send_sem, recv_sem, ep, to * NC + tc)

    def along(dy):
        return (ty + dy) % NY

    def from_sources(y, q, recv_sem):
        @pl.when(own_q == q)
        def _():
            arrived(gath.at[y, q, pl.ds(0, chunk_rows - block)], recv_sem.at[q])

        @pl.when(own_q != q)
        def _():
            arrived(gath.at[y, q], recv_sem.at[q])

    def stage_a(q):
        from_sources(ty, q, disp_recv)
        share_out(gath, ty, q, ag_send, ag_recv.at[ty, q], along(1))
        share_out(gath, ty, q, ag_send, ag_recv.at[ty, q], along(3))

    def stage_d(q):
        from_sources(far, q, far_recv)
        for dy in (1, 3):
            arrived(gath.at[along(dy), q], ag_recv.at[along(dy), q])
        parts = []
        for y in range(NY):
            both = gath[y, q].astype(F32).reshape(PER, NC, cap, share)
            parts += [both[:, i].reshape(work_rows, share).astype(BF16) for i in range(NC)]
        x = jnp.concatenate(parts, axis=-1)
        both = jnp.dot(x, columns[...], preferred_element_type=F32)
        g, u = both[:, : NC * half], both[:, NC * half :]
        hid[ty, q] = (g / (1.0 + jnp.exp(-g)) * u).astype(BF16)
        for dy in (2, 1, 3):
            share_out(hid, ty, q, hid_send, hid_recv.at[q], along(dy))

    def stage_f(q):
        if q == 0:
            load_down.wait()
            arrived(wd.at[pl.ds(0, NT - 1)], wd_recv)
        arrived(hid.at[pl.ds(0, NY - 1), q], hid_recv.at[q])
        x = jnp.concatenate([hid[y, q] for y in range(NY)], axis=-1)
        result = jnp.dot(x, wd[...].reshape(NT * half, quarter), preferred_element_type=F32)
        top = jnp.maximum(jnp.max(jnp.abs(result), axis=-1, keepdims=True), 1e-30)
        key = jnp.ceil(jnp.log2(top) * KEYS) + 1.0
        level = jnp.round(result * (LEVELS * jnp.exp2(key * (-1.0 / KEYS)))).astype(jnp.int32)
        for c in range(NC):
            left = level[:, c * share : c * share + 128]
            right = level[:, c * share + 128 : (c + 1) * share]
            outb[pl.ds(c * NE + q * PER, PER), 0:cap, :] = ((left << 16) | (right & 0xFFFF)).reshape(PER, cap, 128)
        row = lax.broadcasted_iota(jnp.int32, (work_rows, 128), 0) % cap
        col = lax.broadcasted_iota(jnp.int32, (work_rows, 128), 1)
        keys = jnp.where(col == row + ep % (128 // cap) * cap, key, 0.0)
        keys = jnp.sum(keys.reshape(PER, cap, 128), axis=1, keepdims=True).astype(jnp.int32)
        for c in range(NC):
            outb[pl.ds(c * NE + q * PER, PER), cap : cap + 1, :] = keys

        @pl.when(own_q == q)
        def _():
            r = own_line % LINES * NX + ex
            ret[tc, ep] = outb[tc * NE + q * PER + r]

        for k in range(LINES):
            line = q * LINES + k
            z = ZORDER[line] if ABSOLUTE else (ez + ORDER[line]) % NZ

            @pl.loop(0, NX)
            def _(x):
                e, r = z * NX + x, k * NX + x
                for c in range(NC):

                    @pl.when((e != ep) | (c != tc))
                    def _():
                        t = ty * NC + c
                        send(outb.at[c * NE + q * PER + r], ret.at[tc, ep], ret_send, ret_recv.at[tc], e, t)

    stages = {"a": stage_a, "d": stage_d, "f": stage_f}
    for word in SEQ:
        with jax.named_scope(f"stage_{word}"):
            stages[word[0]](int(word[1:]))

    per = 128 // cap
    total = jnp.zeros(out_v.shape, F32)
    for c in (1, 0):
        with jax.named_scope(f"ret_wait{c}"):

            @pl.when(tc == c)
            def _():
                arrived(ret.at[c, pl.ds(0, NE - 1)], ret_recv.at[c])

            @pl.when(tc != c)
            def _():
                arrived(ret.at[c], ret_recv.at[c])

        words = ret[c, :, 0:cap, :].reshape(NE * cap, 128)
        back = jnp.concatenate([words >> 16, (words << 16) >> 16], axis=-1)
        keys = ret[c, :, cap : cap + 1, :].astype(F32)
        keys = jnp.concatenate([jnp.sum(keys[i : i + per], axis=0) for i in range(0, NE, per)], axis=-1)
        scale = jnp.exp2(keys * (1.0 / KEYS)) * (1.0 / LEVELS)
        total = total + weighted(combine[c] * scale, back)
    out_v[...] = total.astype(out_v.dtype)

    with jax.named_scope("drain"):
        arrived(packed.at[pl.ds(0, (NE - 1) * block)], disp_send)
        arrived(wd.at[pl.ds(0, NT - 1)], wd_send)
        arrived(wall.at[0], wall_send)
        arrived(gath.at[pl.ds(0, 2)], ag_send)
        arrived(packed.at[pl.ds(0, (NE - 1) * block)], far_send)
        arrived(hid.at[pl.ds(0, NY - 1)], hid_send)
        arrived(outb.at[pl.ds(0, NE * NC - 1)], ret_send)


def per_device(tokens, norm_gain, norm_shift, expert_ids, gate_weights, expert_gate, expert_up, expert_down):
    rows, features = tokens.shape
    local, _, half = expert_gate.shape
    quarter = features // NY
    share = features // NT
    cap = rows // 2 * expert_ids.shape[1] // (local * NE // GROUPS)
    block = local * cap
    any_spec = pl.BlockSpec(memory_space=pl.ANY)
    vmem = pl.BlockSpec(memory_space=pltpu.VMEM)
    dma = pltpu.SemaphoreType.DMA
    out = pl.pallas_call(
        kernel,
        out_shape=pltpu.VMEM((rows, share), F32),
        in_specs=[any_spec, vmem, vmem, vmem, vmem, any_spec, any_spec, any_spec],
        out_specs=vmem,
        scratch_shapes=[
            pltpu.VMEM((rows, features), BF16),
            pltpu.VMEM((2, NC, half, features), BF16),
            pltpu.VMEM((features, 2 * NC * half), BF16),
            pltpu.VMEM((NE * block, share), BF16),
            pltpu.VMEM((NE * block, share), BF16),
            pltpu.VMEM((NY, CHUNKS, PER * block, share), BF16),
            pltpu.VMEM((NT, half, quarter), BF16),
            pltpu.VMEM((NY, CHUNKS, PER * cap, NC * half), BF16),
            pltpu.VMEM((NE * NC, cap + 1, 128), jnp.int32),
            pltpu.VMEM((NC, NE, cap + 1, 128), jnp.int32),
            pltpu.VMEM((NC, rows, NE * cap), F32),
            dma((4,)),
            dma,
            dma((CHUNKS,)),
            dma,
            dma((CHUNKS,)),
            dma,
            dma((NY, CHUNKS)),
            dma,
            dma,
            dma,
            dma,
            dma,
            dma((CHUNKS,)),
            dma,
            dma((NC,)),
        ],
        compiler_params=pltpu.CompilerParams(collective_id=0, has_side_effects=True, vmem_limit_bytes=VMEM_LIMIT),
    )(
        tokens,
        norm_gain.reshape(1, features),
        norm_shift.reshape(1, features),
        expert_ids.T,
        gate_weights.T,
        expert_gate.transpose(0, 2, 1),
        expert_up.transpose(0, 2, 1),
        expert_down,
    )
    return out.astype(BF16)


def solution(mesh):
    return jax.shard_map(
        per_device,
        mesh=mesh,
        in_specs=(
            P("ep", None),
            P(),
            P(),
            P("ep", None),
            P("ep", None),
            P("ep", None, "tp"),
            P("ep", None, "tp"),
            P("ep", "tp", None),
        ),
        out_specs=P("ep", "tp"),
        check_vma=False,
    )
```

```python
import jax
import jax.numpy as jnp
from jax import lax
from jax.experimental import pallas as pl
from jax.experimental.pallas import tpu as pltpu
from jax.sharding import PartitionSpec as P

MESH = pl.DeviceIdType.MESH
GROUPS = 4
NZ, NX, NY, NC = 8, 4, 4, 2
NE, NT = NZ * NX, NY * NC
ABSOLUTE = True
ZORDER = (0, 4, 1, 5, 2, 6, 3, 7)
SEND_FAR = True
SIG_FAR = True
ORDER = (0, 7, 1, 6, 2, 5, 3, 4)
CHUNKS = 4
LINES = NZ // CHUNKS
PER = NE // CHUNKS
FAR_AT = 1
WD_AT = 0
FAR_FAR = True
SEQ = ("a0", "a1", "a2", "a3", "d0", "d1", "d2", "d3", "f0", "f1", "f2", "f3")
FINAL_CAST = True
VMEM_LIMIT = 56 * 2**20
epsilon = 1e-05
LEVELS = 32760.0
KEYS = 128.0
F32, BF16 = jnp.float32, jnp.bfloat16


def weighted(weights, codes):
    high = (codes + 128) >> 8
    low = codes - (high << 8)
    parts, rest = [], weights
    for _ in range(3):
        parts.append(rest.astype(BF16))
        rest = rest - parts[-1].astype(F32)
    left = jnp.concatenate(parts, axis=0)
    right = jnp.concatenate([high.astype(F32).astype(BF16), low.astype(F32).astype(BF16)], axis=-1)
    terms = jnp.dot(left, right, preferred_element_type=F32)
    n, m = weights.shape[0], codes.shape[1]
    terms = terms[:n] + terms[n : 2 * n] + terms[2 * n :]
    return terms[:, :m] * 256.0 + terms[:, m:]


def kernel(
    tokens_h, gain_v, shift_v, ids_v, gw_v, gate_h, up_h, down_h, out_v,
    tok, wall, columns, packed, spare, gath, wd, hid, outb, ret, combine,
    load_sem, disp_send, disp_recv, far_send, far_recv, ag_send, ag_recv, wall_send, wall_recv, wd_send, wd_recv, hid_send, hid_recv,
    ret_send, ret_recv,
):
    ep, tp = lax.axis_index("ep"), lax.axis_index("tp")
    ez, ex = ep // NX, ep % NX
    ty, tc = tp // NC, tp % NC
    mate = ty * NC + 1 - tc
    rows, features = tok.shape
    quarter = features // NY
    share = quarter // NC
    block = packed.shape[0] // NE
    cap = block // NC
    half = wall.shape[2]
    chunk_rows = PER * block
    work_rows = PER * cap
    own_line = sum(jnp.where(ez == z, line, 0) for line, z in enumerate(ZORDER)) if ABSOLUTE else ORDER.index(0)
    own_q = own_line // LINES

    def arrived(ref, sem):
        pltpu.make_async_copy(ref, ref, sem).wait()

    def send(src, dst, send_sem, recv_sem, e, t):
        pltpu.make_async_remote_copy(
            src_ref=src, dst_ref=dst, send_sem=send_sem, recv_sem=recv_sem, device_id=(e, t), device_id_type=MESH
        ).start()

    def rows_of(n):
        return pl.ds(pl.multiple_of(n * block, block), block)

    def quarter_of(y):
        return pl.ds(pl.multiple_of(y * quarter, quarter), quarter)

    load_tok = pltpu.make_async_copy(tokens_h, tok, load_sem.at[0])
    load_gate = pltpu.make_async_copy(gate_h.at[tc], wall.at[0, tc], load_sem.at[1])
    load_up = pltpu.make_async_copy(up_h.at[tc], wall.at[1, tc], load_sem.at[2])
    load_down = pltpu.make_async_copy(down_h.at[tc, :, quarter_of(ty)], wd.at[tp], load_sem.at[3])
    load_tok.start()

    barrier = pltpu.get_barrier_semaphore()

    def signal(e, t):
        pl.semaphore_signal(barrier, inc=1, device_id=(e, t), device_id_type=MESH)

    for dz in (0, 1, 7, 2, 6, 3, 5, 4):
        for dx in range(1 if dz == 0 else 0, NX):
            signal(((ez + dz) % NZ) * NX + (ex + dx) % NX, tp)
    for d in (2, 4, 6, 1, 3, 5, 7):
        signal(ep, (tp + d) % NT)

    ids, gw = ids_v[...], gw_v[...]
    earlier = lax.broadcasted_iota(jnp.int32, (rows, rows), 0) < lax.broadcasted_iota(jnp.int32, (rows, rows), 1)
    earlier = jnp.where(earlier, 1.0, 0.0).astype(BF16)

    def placed(numbers):
        hits = jnp.zeros(numbers.shape, F32)
        weights = jnp.zeros(numbers.shape, F32)
        for k in range(ids.shape[0]):
            same = ids[k : k + 1, :] == numbers
            hits = hits + jnp.where(same, 1.0, 0.0)
            weights = weights + jnp.where(same, gw[k : k + 1, :], 0.0)
        before = jnp.dot(hits.astype(BF16), earlier, preferred_element_type=F32)
        code = hits * (before + 1.0)
        wanted = (lax.broadcasted_iota(jnp.int32, (numbers.shape[0], cap, rows), 1) + 1).astype(F32)
        return code[:, None, :] == wanted, weights

    with jax.named_scope("p_place"):
        place, _ = placed(lax.broadcasted_iota(jnp.int32, (NE, rows), 0) * NC + tc)
        place = jnp.where(place, 1.0, 0.0).reshape(NE * cap, rows).astype(BF16)

    load_tok.wait()
    load_gate.start()
    load_up.start()
    load_down.start()
    with jax.named_scope("p_ln"):
        values = tok[...].astype(F32)
        centre = jnp.mean(values, axis=-1, keepdims=True)
        spread = jnp.mean(jnp.square(values - centre), axis=-1, keepdims=True)
        scale = lax.rsqrt(spread + epsilon)

        def pack(y, buf):
            own = tok[:, quarter_of(y)].astype(F32)
            normed = (own - centre) * scale * gain_v[:, quarter_of(y)] + shift_v[:, quarter_of(y)]
            picked = jnp.dot(place, normed.astype(BF16), preferred_element_type=F32).reshape(NE, cap, quarter)
            picked = jnp.stack([picked[:, :, :share], picked[:, :, share:]], axis=1)
            buf[...] = picked.reshape(NE * block, share).astype(BF16)
            gath[y, own_q, rows_of(own_line % LINES * NX + ex), :] = buf[rows_of(ep), :]

        pack(ty, packed)

    with jax.named_scope("entry_wait"):
        pl.semaphore_wait(barrier, NE - 1 + NT - 1)

    def dispatch(buf, y, send_sem, recv_sem, farthest=SEND_FAR):
        sends = tuple(enumerate(ORDER))
        for line, dz in reversed(sends) if farthest else sends:
            line = own_line if ABSOLUTE else line

            @pl.loop(1 if dz == 0 else 0, NX)
            def _(dx):
                e = ((ez + NZ - dz) % NZ) * NX + (ex + dx) % NX
                send(
                    buf.at[rows_of(e)], gath.at[y, line // LINES, rows_of(line % LINES * NX + ex)],
                    send_sem, recv_sem.at[line // LINES], e, tp,
                )

    dispatch(packed, ty, disp_send, disp_recv)

    def exchange_down():
        for d in (2, 4, 6, 1, 3, 5, 7):
            t = (tp + d) % NT
            send(down_h.at[t % NC, :, quarter_of(t // NC)], wd.at[tp], wd_send, wd_recv, ep, t)

    if WD_AT == 0:
        exchange_down()

    send(gate_h.at[1 - tc], wall.at[0, tc], wall_send, wall_recv, ep, mate)
    send(up_h.at[1 - tc], wall.at[1, tc], wall_send, wall_recv, ep, mate)

    far = (ty + 2) % NY
    if FAR_AT == 0:
        pack(far, spare)
        dispatch(spare, far, far_send, far_recv, FAR_FAR)

    with jax.named_scope("p_combine"):
        number = lax.broadcasted_iota(jnp.int32, (NE * NC, rows), 0)
        every, weights = placed(number % NE * NC + number // NE)
        w_slots = jnp.where(every, weights[:, None, :], 0.0).reshape(NE * block, rows)
        for c in range(NC):
            combine[c] = w_slots[c * NE * cap : (c + 1) * NE * cap].T

    if WD_AT == 1:
        exchange_down()
    if FAR_AT == 2:
        pack(far, spare)
        dispatch(spare, far, far_send, far_recv, FAR_FAR)

    with jax.named_scope("p_columns"):
        load_gate.wait()
        load_up.wait()
        arrived(wall.at[0], wall_recv)
        for i in range(0, features, quarter):
            columns[i : i + quarter, :] = wall[:, :, :, i : i + quarter].reshape(2 * NC * half, quarter).T

    if FAR_AT == 1:
        pack(far, spare)
        dispatch(spare, far, far_send, far_recv, FAR_FAR)

    def share_out(buf, y, q, send_sem, recv_sem, to, part=None):
        ref = buf.at[y, q] if part is None else buf.at[y, q, part]
        send(ref, ref, send_sem, recv_sem, ep, to * NC + tc)

    def along(dy):
        return (ty + dy) % NY

    def from_sources(y, q, recv_sem):
        @pl.when(own_q == q)
        def _():
            arrived(gath.at[y, q, pl.ds(0, chunk_rows - block)], recv_sem.at[q])

        @pl.when(own_q != q)
        def _():
            arrived(gath.at[y, q], recv_sem.at[q])

    def stage_a(q):
        from_sources(ty, q, disp_recv)
        share_out(gath, ty, q, ag_send, ag_recv.at[ty, q], along(1))
        share_out(gath, ty, q, ag_send, ag_recv.at[ty, q], along(3))

    def stage_d(q):
        from_sources(far, q, far_recv)
        for dy in (1, 3):
            arrived(gath.at[along(dy), q], ag_recv.at[along(dy), q])
        parts = []
        for y in range(NY):
            both = gath[y, q].astype(F32).reshape(PER, NC, cap, share)
            parts += [both[:, i].reshape(work_rows, share).astype(BF16) for i in range(NC)]
        x = jnp.concatenate(parts, axis=-1)
        both = jnp.dot(x, columns[...], preferred_element_type=F32)
        g, u = both[:, : NC * half], both[:, NC * half :]
        hid[ty, q] = (g / (1.0 + jnp.exp(-g)) * u).astype(BF16)
        for dy in (2, 1, 3):
            share_out(hid, ty, q, hid_send, hid_recv.at[q], along(dy))

    def stage_f(q):
        if q == 0:
            load_down.wait()
            arrived(wd.at[pl.ds(0, NT - 1)], wd_recv)
        arrived(hid.at[pl.ds(0, NY - 1), q], hid_recv.at[q])
        x = jnp.concatenate([hid[y, q] for y in range(NY)], axis=-1)
        result = jnp.dot(x, wd[...].reshape(NT * half, quarter), preferred_element_type=F32)
        top = jnp.maximum(jnp.max(jnp.abs(result), axis=-1, keepdims=True), 1e-30)
        key = jnp.ceil(jnp.log2(top) * KEYS) + 1.0
        level = jnp.round(result * (LEVELS * jnp.exp2(key * (-1.0 / KEYS)))).astype(jnp.int32)
        for c in range(NC):
            left = level[:, c * share : c * share + 128]
            right = level[:, c * share + 128 : (c + 1) * share]
            outb[pl.ds(c * NE + q * PER, PER), 0:cap, :] = ((left << 16) | (right & 0xFFFF)).reshape(PER, cap, 128)
        row = lax.broadcasted_iota(jnp.int32, (work_rows, 128), 0) % cap
        col = lax.broadcasted_iota(jnp.int32, (work_rows, 128), 1)
        keys = jnp.where(col == row + ep % (128 // cap) * cap, key, 0.0)
        keys = jnp.sum(keys.reshape(PER, cap, 128), axis=1, keepdims=True).astype(jnp.int32)
        for c in range(NC):
            outb[pl.ds(c * NE + q * PER, PER), cap : cap + 1, :] = keys

        @pl.when(own_q == q)
        def _():
            r = own_line % LINES * NX + ex
            ret[tc, ep] = outb[tc * NE + q * PER + r]

        for k in range(LINES):
            line = q * LINES + k
            z = ZORDER[line] if ABSOLUTE else (ez + ORDER[line]) % NZ

            @pl.loop(0, NX)
            def _(x):
                e, r = z * NX + x, k * NX + x
                for c in range(NC):

                    @pl.when((e != ep) | (c != tc))
                    def _():
                        t = ty * NC + c
                        send(outb.at[c * NE + q * PER + r], ret.at[tc, ep], ret_send, ret_recv.at[tc], e, t)

    stages = {"a": stage_a, "d": stage_d, "f": stage_f}
    for word in SEQ:
        with jax.named_scope(f"stage_{word}"):
            stages[word[0]](int(word[1:]))

    per = 128 // cap
    total = jnp.zeros(out_v.shape, F32)
    for c in (1, 0):
        with jax.named_scope(f"ret_wait{c}"):

            @pl.when(tc == c)
            def _():
                arrived(ret.at[c, pl.ds(0, NE - 1)], ret_recv.at[c])

            @pl.when(tc != c)
            def _():
                arrived(ret.at[c], ret_recv.at[c])

        words = ret[c, :, 0:cap, :].reshape(NE * cap, 128)
        back = jnp.concatenate([words >> 16, (words << 16) >> 16], axis=-1)
        keys = ret[c, :, cap : cap + 1, :].astype(F32)
        keys = jnp.concatenate([jnp.sum(keys[i : i + per], axis=0) for i in range(0, NE, per)], axis=-1)
        scale = jnp.exp2(keys * (1.0 / KEYS)) * (1.0 / LEVELS)
        total = total + weighted(combine[c] * scale, back)
    out_v[...] = total.astype(out_v.dtype)

    with jax.named_scope("drain"):
        arrived(packed.at[pl.ds(0, (NE - 1) * block)], disp_send)
        arrived(wd.at[pl.ds(0, NT - 1)], wd_send)
        arrived(wall.at[0], wall_send)
        arrived(gath.at[pl.ds(0, 2)], ag_send)
        arrived(packed.at[pl.ds(0, (NE - 1) * block)], far_send)
        arrived(hid.at[pl.ds(0, NY - 1)], hid_send)
        arrived(outb.at[pl.ds(0, NE * NC - 1)], ret_send)


def per_device(tokens, norm_gain, norm_shift, expert_ids, gate_weights, expert_gate, expert_up, expert_down):
    rows, features = tokens.shape
    local, _, half = expert_gate.shape
    quarter = features // NY
    share = features // NT
    cap = rows // 2 * expert_ids.shape[1] // (local * NE // GROUPS)
    block = local * cap
    any_spec = pl.BlockSpec(memory_space=pl.ANY)
    vmem = pl.BlockSpec(memory_space=pltpu.VMEM)
    dma = pltpu.SemaphoreType.DMA
    out = pl.pallas_call(
        kernel,
        out_shape=pltpu.VMEM((rows, share), F32),
        in_specs=[any_spec, vmem, vmem, vmem, vmem, any_spec, any_spec, any_spec],
        out_specs=vmem,
        scratch_shapes=[
            pltpu.VMEM((rows, features), BF16),
            pltpu.VMEM((2, NC, half, features), BF16),
            pltpu.VMEM((features, 2 * NC * half), BF16),
            pltpu.VMEM((NE * block, share), BF16),
            pltpu.VMEM((NE * block, share), BF16),
            pltpu.VMEM((NY, CHUNKS, PER * block, share), BF16),
            pltpu.VMEM((NT, half, quarter), BF16),
            pltpu.VMEM((NY, CHUNKS, PER * cap, NC * half), BF16),
            pltpu.VMEM((NE * NC, cap + 1, 128), jnp.int32),
            pltpu.VMEM((NC, NE, cap + 1, 128), jnp.int32),
            pltpu.VMEM((NC, rows, NE * cap), F32),
            dma((4,)),
            dma,
            dma((CHUNKS,)),
            dma,
            dma((CHUNKS,)),
            dma,
            dma((NY, CHUNKS)),
            dma,
            dma,
            dma,
            dma,
            dma,
            dma((CHUNKS,)),
            dma,
            dma((NC,)),
        ],
        compiler_params=pltpu.CompilerParams(collective_id=0, has_side_effects=True, vmem_limit_bytes=VMEM_LIMIT),
    )(
        tokens,
        norm_gain.reshape(1, features),
        norm_shift.reshape(1, features),
        expert_ids.T,
        gate_weights.T,
        expert_gate.transpose(0, 2, 1),
        expert_up.transpose(0, 2, 1),
        expert_down,
    )
    return out.astype(BF16)


def solution(mesh):
    return jax.shard_map(
        per_device,
        mesh=mesh,
        in_specs=(
            P("ep", None),
            P(),
            P(),
            P("ep", None),
            P("ep", None),
            P("ep", None, "tp"),
            P("ep", None, "tp"),
            P("ep", "tp", None),
        ),
        out_specs=P("ep", "tp"),
        check_vma=False,
    )
```

```python
import jax
import jax.numpy as jnp
from jax import lax
from jax.experimental import pallas as pl
from jax.experimental.pallas import tpu as pltpu
from jax.sharding import PartitionSpec as P

MESH = pl.DeviceIdType.MESH
GROUPS = 4
NZ, NX, NY, NC = 8, 4, 4, 2
NE, NT = NZ * NX, NY * NC
ABSOLUTE = True
ZORDER = (0, 4, 1, 5, 2, 6, 3, 7)
SEND_FAR = True
SIG_FAR = True
ORDER = (0, 7, 1, 6, 2, 5, 3, 4)
CHUNKS = 4
LINES = NZ // CHUNKS
PER = NE // CHUNKS
FAR_AT = 1
WD_AT = 0
FAR_FAR = True
SEQ = ("a0", "a1", "a2", "a3", "d0", "d1", "d2", "d3", "f0", "f1", "f2", "f3")
FINAL_CAST = True
VMEM_LIMIT = 56 * 2**20
epsilon = 1e-05
LEVELS = 32760.0
KEYS = 128.0
F32, BF16 = jnp.float32, jnp.bfloat16


def weighted(weights, codes):
    high = (codes + 128) >> 8
    low = codes - (high << 8)
    parts, rest = [], weights
    for _ in range(3):
        parts.append(rest.astype(BF16))
        rest = rest - parts[-1].astype(F32)
    left = jnp.concatenate(parts, axis=0)
    right = jnp.concatenate([high.astype(F32).astype(BF16), low.astype(F32).astype(BF16)], axis=-1)
    terms = jnp.dot(left, right, preferred_element_type=F32)
    n, m = weights.shape[0], codes.shape[1]
    terms = terms[:n] + terms[n : 2 * n] + terms[2 * n :]
    return terms[:, :m] * 256.0 + terms[:, m:]


def kernel(
    tokens_h, gain_v, shift_v, ids_v, gw_v, gate_h, up_h, down_h, out_v,
    tok, wall, columns, packed, spare, gath, wd, hid, outb, ret, combine,
    load_sem, disp_send, disp_recv, far_send, far_recv, ag_send, ag_recv, wall_send, wall_recv, wd_send, wd_recv, hid_send, hid_recv,
    ret_send, ret_recv,
):
    ep, tp = lax.axis_index("ep"), lax.axis_index("tp")
    ez, ex = ep // NX, ep % NX
    ty, tc = tp // NC, tp % NC
    mate = ty * NC + 1 - tc
    rows, features = tok.shape
    quarter = features // NY
    share = quarter // NC
    block = packed.shape[0] // NE
    cap = block // NC
    half = wall.shape[2]
    chunk_rows = PER * block
    work_rows = PER * cap
    own_line = sum(jnp.where(ez == z, line, 0) for line, z in enumerate(ZORDER)) if ABSOLUTE else ORDER.index(0)
    own_q = own_line // LINES

    def arrived(ref, sem):
        pltpu.make_async_copy(ref, ref, sem).wait()

    def send(src, dst, send_sem, recv_sem, e, t):
        pltpu.make_async_remote_copy(
            src_ref=src, dst_ref=dst, send_sem=send_sem, recv_sem=recv_sem, device_id=(e, t), device_id_type=MESH
        ).start()

    def rows_of(n):
        return pl.ds(pl.multiple_of(n * block, block), block)

    def quarter_of(y):
        return pl.ds(pl.multiple_of(y * quarter, quarter), quarter)

    load_tok = pltpu.make_async_copy(tokens_h, tok, load_sem.at[0])
    load_gate = pltpu.make_async_copy(gate_h.at[tc], wall.at[0, tc], load_sem.at[1])
    load_up = pltpu.make_async_copy(up_h.at[tc], wall.at[1, tc], load_sem.at[2])
    load_down = pltpu.make_async_copy(down_h.at[tc, :, quarter_of(ty)], wd.at[tp], load_sem.at[3])
    load_tok.start()

    barrier = pltpu.get_barrier_semaphore()

    def signal(e, t):
        pl.semaphore_signal(barrier, inc=1, device_id=(e, t), device_id_type=MESH)

    for dz in (0, 1, 7, 2, 6, 3, 5, 4):
        for dx in range(1 if dz == 0 else 0, NX):
            signal(((ez + dz) % NZ) * NX + (ex + dx) % NX, tp)
    for d in (2, 4, 6, 1, 3, 5, 7):
        signal(ep, (tp + d) % NT)

    ids, gw = ids_v[...], gw_v[...]
    earlier = lax.broadcasted_iota(jnp.int32, (rows, rows), 0) < lax.broadcasted_iota(jnp.int32, (rows, rows), 1)
    earlier = jnp.where(earlier, 1.0, 0.0).astype(BF16)

    def placed(numbers):
        hits = jnp.zeros(numbers.shape, F32)
        weights = jnp.zeros(numbers.shape, F32)
        for k in range(ids.shape[0]):
            same = ids[k : k + 1, :] == numbers
            hits = hits + jnp.where(same, 1.0, 0.0)
            weights = weights + jnp.where(same, gw[k : k + 1, :], 0.0)
        before = jnp.dot(hits.astype(BF16), earlier, preferred_element_type=F32)
        code = hits * (before + 1.0)
        wanted = (lax.broadcasted_iota(jnp.int32, (numbers.shape[0], cap, rows), 1) + 1).astype(F32)
        return code[:, None, :] == wanted, weights

    with jax.named_scope("p_place"):
        place, _ = placed(lax.broadcasted_iota(jnp.int32, (NE, rows), 0) * NC + tc)
        place = jnp.where(place, 1.0, 0.0).reshape(NE * cap, rows).astype(BF16)

    load_tok.wait()
    load_gate.start()
    load_up.start()
    load_down.start()
    with jax.named_scope("p_ln"):
        values = tok[...].astype(F32)
        centre = jnp.mean(values, axis=-1, keepdims=True)
        spread = jnp.mean(jnp.square(values - centre), axis=-1, keepdims=True)
        scale = lax.rsqrt(spread + epsilon)

        def pack(y, buf):
            own = tok[:, quarter_of(y)].astype(F32)
            normed = (own - centre) * scale * gain_v[:, quarter_of(y)] + shift_v[:, quarter_of(y)]
            picked = jnp.dot(place, normed.astype(BF16), preferred_element_type=F32).reshape(NE, cap, quarter)
            picked = jnp.stack([picked[:, :, :share], picked[:, :, share:]], axis=1)
            buf[...] = picked.reshape(NE * block, share).astype(BF16)
            gath[y, own_q, rows_of(own_line % LINES * NX + ex), :] = buf[rows_of(ep), :]

        pack(ty, packed)

    with jax.named_scope("entry_wait"):
        pl.semaphore_wait(barrier, NE - 1 + NT - 1)

    def dispatch(buf, y, send_sem, recv_sem, farthest=SEND_FAR):
        sends = tuple(enumerate(ORDER))
        for line, dz in reversed(sends) if farthest else sends:
            line = own_line if ABSOLUTE else line

            @pl.loop(1 if dz == 0 else 0, NX)
            def _(dx):
                e = ((ez + NZ - dz) % NZ) * NX + (ex + dx) % NX
                send(
                    buf.at[rows_of(e)], gath.at[y, line // LINES, rows_of(line % LINES * NX + ex)],
                    send_sem, recv_sem.at[line // LINES], e, tp,
                )

    dispatch(packed, ty, disp_send, disp_recv)

    def exchange_down():
        for d in (2, 4, 6, 1, 3, 5, 7):
            t = (tp + d) % NT
            send(down_h.at[t % NC, :, quarter_of(t // NC)], wd.at[tp], wd_send, wd_recv, ep, t)

    if WD_AT == 0:
        exchange_down()

    send(gate_h.at[1 - tc], wall.at[0, tc], wall_send, wall_recv, ep, mate)
    send(up_h.at[1 - tc], wall.at[1, tc], wall_send, wall_recv, ep, mate)

    far = (ty + 2) % NY
    if FAR_AT == 0:
        pack(far, spare)
        dispatch(spare, far, far_send, far_recv, FAR_FAR)

    with jax.named_scope("p_combine"):
        number = lax.broadcasted_iota(jnp.int32, (NE * NC, rows), 0)
        every, weights = placed(number % NE * NC + number // NE)
        w_slots = jnp.where(every, weights[:, None, :], 0.0).reshape(NE * block, rows)
        for c in range(NC):
            combine[c] = w_slots[c * NE * cap : (c + 1) * NE * cap].T

    if WD_AT == 1:
        exchange_down()
    if FAR_AT == 2:
        pack(far, spare)
        dispatch(spare, far, far_send, far_recv, FAR_FAR)

    with jax.named_scope("p_columns"):
        load_gate.wait()
        load_up.wait()
        arrived(wall.at[0], wall_recv)
        for i in range(0, features, quarter):
            columns[i : i + quarter, :] = wall[:, :, :, i : i + quarter].reshape(2 * NC * half, quarter).T

    if FAR_AT == 1:
        pack(far, spare)
        dispatch(spare, far, far_send, far_recv, FAR_FAR)

    def share_out(buf, y, q, send_sem, recv_sem, to, part=None):
        ref = buf.at[y, q] if part is None else buf.at[y, q, part]
        send(ref, ref, send_sem, recv_sem, ep, to * NC + tc)

    def along(dy):
        return (ty + dy) % NY

    def from_sources(y, q, recv_sem):
        @pl.when(own_q == q)
        def _():
            arrived(gath.at[y, q, pl.ds(0, chunk_rows - block)], recv_sem.at[q])

        @pl.when(own_q != q)
        def _():
            arrived(gath.at[y, q], recv_sem.at[q])

    def stage_a(q):
        from_sources(ty, q, disp_recv)
        share_out(gath, ty, q, ag_send, ag_recv.at[ty, q], along(3))
        share_out(gath, ty, q, ag_send, ag_recv.at[ty, q], along(1))

    def stage_d(q):
        from_sources(far, q, far_recv)
        for dy in (1, 3):
            arrived(gath.at[along(dy), q], ag_recv.at[along(dy), q])
        parts = []
        for y in range(NY):
            both = gath[y, q].astype(F32).reshape(PER, NC, cap, share)
            parts += [both[:, i].reshape(work_rows, share).astype(BF16) for i in range(NC)]
        x = jnp.concatenate(parts, axis=-1)
        both = jnp.dot(x, columns[...], preferred_element_type=F32)
        g, u = both[:, : NC * half], both[:, NC * half :]
        hid[ty, q] = (g / (1.0 + jnp.exp(-g)) * u).astype(BF16)
        for dy in (2, 1, 3):
            share_out(hid, ty, q, hid_send, hid_recv.at[q], along(dy))

    def stage_f(q):
        if q == 0:
            load_down.wait()
            arrived(wd.at[pl.ds(0, NT - 1)], wd_recv)
        arrived(hid.at[pl.ds(0, NY - 1), q], hid_recv.at[q])
        x = jnp.concatenate([hid[y, q] for y in range(NY)], axis=-1)
        result = jnp.dot(x, wd[...].reshape(NT * half, quarter), preferred_element_type=F32)
        top = jnp.maximum(jnp.max(jnp.abs(result), axis=-1, keepdims=True), 1e-30)
        key = jnp.ceil(jnp.log2(top) * KEYS) + 1.0
        level = jnp.round(result * (LEVELS * jnp.exp2(key * (-1.0 / KEYS)))).astype(jnp.int32)
        for c in range(NC):
            left = level[:, c * share : c * share + 128]
            right = level[:, c * share + 128 : (c + 1) * share]
            outb[pl.ds(c * NE + q * PER, PER), 0:cap, :] = ((left << 16) | (right & 0xFFFF)).reshape(PER, cap, 128)
        row = lax.broadcasted_iota(jnp.int32, (work_rows, 128), 0) % cap
        col = lax.broadcasted_iota(jnp.int32, (work_rows, 128), 1)
        keys = jnp.where(col == row + ep % (128 // cap) * cap, key, 0.0)
        keys = jnp.sum(keys.reshape(PER, cap, 128), axis=1, keepdims=True).astype(jnp.int32)
        for c in range(NC):
            outb[pl.ds(c * NE + q * PER, PER), cap : cap + 1, :] = keys

        @pl.when(own_q == q)
        def _():
            r = own_line % LINES * NX + ex
            ret[tc, ep] = outb[tc * NE + q * PER + r]

        for k in range(LINES):
            line = q * LINES + k
            z = ZORDER[line] if ABSOLUTE else (ez + ORDER[line]) % NZ

            @pl.loop(0, NX)
            def _(x):
                e, r = z * NX + x, k * NX + x
                for c in range(NC):

                    @pl.when((e != ep) | (c != tc))
                    def _():
                        t = ty * NC + c
                        send(outb.at[c * NE + q * PER + r], ret.at[tc, ep], ret_send, ret_recv.at[tc], e, t)

    stages = {"a": stage_a, "d": stage_d, "f": stage_f}
    for word in SEQ:
        with jax.named_scope(f"stage_{word}"):
            stages[word[0]](int(word[1:]))

    per = 128 // cap
    total = jnp.zeros(out_v.shape, F32)
    for c in (1, 0):
        with jax.named_scope(f"ret_wait{c}"):

            @pl.when(tc == c)
            def _():
                arrived(ret.at[c, pl.ds(0, NE - 1)], ret_recv.at[c])

            @pl.when(tc != c)
            def _():
                arrived(ret.at[c], ret_recv.at[c])

        words = ret[c, :, 0:cap, :].reshape(NE * cap, 128)
        back = jnp.concatenate([words >> 16, (words << 16) >> 16], axis=-1)
        keys = ret[c, :, cap : cap + 1, :].astype(F32)
        keys = jnp.concatenate([jnp.sum(keys[i : i + per], axis=0) for i in range(0, NE, per)], axis=-1)
        scale = jnp.exp2(keys * (1.0 / KEYS)) * (1.0 / LEVELS)
        total = total + weighted(combine[c] * scale, back)
    out_v[...] = total.astype(out_v.dtype)

    with jax.named_scope("drain"):
        arrived(packed.at[pl.ds(0, (NE - 1) * block)], disp_send)
        arrived(wd.at[pl.ds(0, NT - 1)], wd_send)
        arrived(wall.at[0], wall_send)
        arrived(gath.at[pl.ds(0, 2)], ag_send)
        arrived(packed.at[pl.ds(0, (NE - 1) * block)], far_send)
        arrived(hid.at[pl.ds(0, NY - 1)], hid_send)
        arrived(outb.at[pl.ds(0, NE * NC - 1)], ret_send)


def per_device(tokens, norm_gain, norm_shift, expert_ids, gate_weights, expert_gate, expert_up, expert_down):
    rows, features = tokens.shape
    local, _, half = expert_gate.shape
    quarter = features // NY
    share = features // NT
    cap = rows // 2 * expert_ids.shape[1] // (local * NE // GROUPS)
    block = local * cap
    any_spec = pl.BlockSpec(memory_space=pl.ANY)
    vmem = pl.BlockSpec(memory_space=pltpu.VMEM)
    dma = pltpu.SemaphoreType.DMA
    out = pl.pallas_call(
        kernel,
        out_shape=pltpu.VMEM((rows, share), F32),
        in_specs=[any_spec, vmem, vmem, vmem, vmem, any_spec, any_spec, any_spec],
        out_specs=vmem,
        scratch_shapes=[
            pltpu.VMEM((rows, features), BF16),
            pltpu.VMEM((2, NC, half, features), BF16),
            pltpu.VMEM((features, 2 * NC * half), BF16),
            pltpu.VMEM((NE * block, share), BF16),
            pltpu.VMEM((NE * block, share), BF16),
            pltpu.VMEM((NY, CHUNKS, PER * block, share), BF16),
            pltpu.VMEM((NT, half, quarter), BF16),
            pltpu.VMEM((NY, CHUNKS, PER * cap, NC * half), BF16),
            pltpu.VMEM((NE * NC, cap + 1, 128), jnp.int32),
            pltpu.VMEM((NC, NE, cap + 1, 128), jnp.int32),
            pltpu.VMEM((NC, rows, NE * cap), F32),
            dma((4,)),
            dma,
            dma((CHUNKS,)),
            dma,
            dma((CHUNKS,)),
            dma,
            dma((NY, CHUNKS)),
            dma,
            dma,
            dma,
            dma,
            dma,
            dma((CHUNKS,)),
            dma,
            dma((NC,)),
        ],
        compiler_params=pltpu.CompilerParams(collective_id=0, has_side_effects=True, vmem_limit_bytes=VMEM_LIMIT),
    )(
        tokens,
        norm_gain.reshape(1, features),
        norm_shift.reshape(1, features),
        expert_ids.T,
        gate_weights.T,
        expert_gate.transpose(0, 2, 1),
        expert_up.transpose(0, 2, 1),
        expert_down,
    )
    return out.astype(BF16)


def solution(mesh):
    return jax.shard_map(
        per_device,
        mesh=mesh,
        in_specs=(
            P("ep", None),
            P(),
            P(),
            P("ep", None),
            P("ep", None),
            P("ep", None, "tp"),
            P("ep", None, "tp"),
            P("ep", "tp", None),
        ),
        out_specs=P("ep", "tp"),
        check_vma=False,
    )
```

```python
import jax
import jax.numpy as jnp
from jax import lax
from jax.experimental import pallas as pl
from jax.experimental.pallas import tpu as pltpu
from jax.sharding import PartitionSpec as P

MESH = pl.DeviceIdType.MESH
GROUPS = 4
NZ, NX, NY, NC = 8, 4, 4, 2
NE, NT = NZ * NX, NY * NC
ABSOLUTE = True
ZORDER = (0, 4, 1, 5, 2, 6, 3, 7)
SEND_FAR = True
SIG_FAR = True
ORDER = (0, 7, 1, 6, 2, 5, 3, 4)
CHUNKS = 4
LINES = NZ // CHUNKS
PER = NE // CHUNKS
FAR_AT = 1
WD_AT = 0
FAR_FAR = True
SEQ = ("a0", "a1", "a2", "a3", "d0", "d1", "d2", "d3", "f0", "f1", "f2", "f3")
FINAL_CAST = True
VMEM_LIMIT = 56 * 2**20
epsilon = 1e-05
LEVELS = 32760.0
KEYS = 128.0
F32, BF16 = jnp.float32, jnp.bfloat16


def weighted(weights, codes):
    high = (codes + 128) >> 8
    low = codes - (high << 8)
    parts, rest = [], weights
    for _ in range(3):
        parts.append(rest.astype(BF16))
        rest = rest - parts[-1].astype(F32)
    left = jnp.concatenate(parts, axis=0)
    right = jnp.concatenate([high.astype(F32).astype(BF16), low.astype(F32).astype(BF16)], axis=-1)
    terms = jnp.dot(left, right, preferred_element_type=F32)
    n, m = weights.shape[0], codes.shape[1]
    terms = terms[:n] + terms[n : 2 * n] + terms[2 * n :]
    return terms[:, :m] * 256.0 + terms[:, m:]


def kernel(
    tokens_h, gain_v, shift_v, ids_v, gw_v, gate_h, up_h, down_h, out_v,
    tok, wall, columns, packed, spare, gath, wd, hid, outb, ret, combine,
    load_sem, disp_send, disp_recv, far_send, far_recv, ag_send, ag_recv, wall_send, wall_recv, wd_send, wd_recv, hid_send, hid_recv,
    ret_send, ret_recv,
):
    ep, tp = lax.axis_index("ep"), lax.axis_index("tp")
    ez, ex = ep // NX, ep % NX
    ty, tc = tp // NC, tp % NC
    mate = ty * NC + 1 - tc
    rows, features = tok.shape
    quarter = features // NY
    share = quarter // NC
    block = packed.shape[0] // NE
    cap = block // NC
    half = wall.shape[2]
    chunk_rows = PER * block
    work_rows = PER * cap
    own_line = sum(jnp.where(ez == z, line, 0) for line, z in enumerate(ZORDER)) if ABSOLUTE else ORDER.index(0)
    own_q = own_line // LINES

    def arrived(ref, sem):
        pltpu.make_async_copy(ref, ref, sem).wait()

    def send(src, dst, send_sem, recv_sem, e, t):
        pltpu.make_async_remote_copy(
            src_ref=src, dst_ref=dst, send_sem=send_sem, recv_sem=recv_sem, device_id=(e, t), device_id_type=MESH
        ).start()

    def rows_of(n):
        return pl.ds(pl.multiple_of(n * block, block), block)

    def quarter_of(y):
        return pl.ds(pl.multiple_of(y * quarter, quarter), quarter)

    load_tok = pltpu.make_async_copy(tokens_h, tok, load_sem.at[0])
    load_gate = pltpu.make_async_copy(gate_h.at[tc], wall.at[0, tc], load_sem.at[1])
    load_up = pltpu.make_async_copy(up_h.at[tc], wall.at[1, tc], load_sem.at[2])
    load_down = pltpu.make_async_copy(down_h.at[tc, :, quarter_of(ty)], wd.at[tp], load_sem.at[3])
    load_tok.start()

    barrier = pltpu.get_barrier_semaphore()

    def signal(e, t):
        pl.semaphore_signal(barrier, inc=1, device_id=(e, t), device_id_type=MESH)

    for dz in (0, 1, 7, 2, 6, 3, 5, 4):
        for dx in range(1 if dz == 0 else 0, NX):
            signal(((ez + dz) % NZ) * NX + (ex + dx) % NX, tp)
    for d in (2, 4, 6, 1, 3, 5, 7):
        signal(ep, (tp + d) % NT)

    ids, gw = ids_v[...], gw_v[...]
    earlier = lax.broadcasted_iota(jnp.int32, (rows, rows), 0) < lax.broadcasted_iota(jnp.int32, (rows, rows), 1)
    earlier = jnp.where(earlier, 1.0, 0.0).astype(BF16)

    def placed(numbers):
        hits = jnp.zeros(numbers.shape, F32)
        weights = jnp.zeros(numbers.shape, F32)
        for k in range(ids.shape[0]):
            same = ids[k : k + 1, :] == numbers
            hits = hits + jnp.where(same, 1.0, 0.0)
            weights = weights + jnp.where(same, gw[k : k + 1, :], 0.0)
        before = jnp.dot(hits.astype(BF16), earlier, preferred_element_type=F32)
        code = hits * (before + 1.0)
        wanted = (lax.broadcasted_iota(jnp.int32, (numbers.shape[0], cap, rows), 1) + 1).astype(F32)
        return code[:, None, :] == wanted, weights

    with jax.named_scope("p_place"):
        place, _ = placed(lax.broadcasted_iota(jnp.int32, (NE, rows), 0) * NC + tc)
        place = jnp.where(place, 1.0, 0.0).reshape(NE * cap, rows).astype(BF16)

    load_tok.wait()
    load_gate.start()
    load_up.start()
    load_down.start()
    with jax.named_scope("p_ln"):
        values = tok[...].astype(F32)
        centre = jnp.mean(values, axis=-1, keepdims=True)
        spread = jnp.mean(jnp.square(values - centre), axis=-1, keepdims=True)
        scale = lax.rsqrt(spread + epsilon)

        def pack(y, buf):
            own = tok[:, quarter_of(y)].astype(F32)
            normed = (own - centre) * scale * gain_v[:, quarter_of(y)] + shift_v[:, quarter_of(y)]
            picked = jnp.dot(place, normed.astype(BF16), preferred_element_type=F32).reshape(NE, cap, quarter)
            picked = jnp.stack([picked[:, :, :share], picked[:, :, share:]], axis=1)
            buf[...] = picked.reshape(NE * block, share).astype(BF16)
            gath[y, own_q, rows_of(own_line % LINES * NX + ex), :] = buf[rows_of(ep), :]

        pack(ty, packed)

    with jax.named_scope("entry_wait"):
        pl.semaphore_wait(barrier, NE - 1 + NT - 1)

    def dispatch(buf, y, send_sem, recv_sem, farthest=SEND_FAR):
        sends = tuple(enumerate(ORDER))
        for line, dz in reversed(sends) if farthest else sends:
            line = own_line if ABSOLUTE else line

            @pl.loop(1 if dz == 0 else 0, NX)
            def _(dx):
                e = ((ez + NZ - dz) % NZ) * NX + (ex + dx) % NX
                send(
                    buf.at[rows_of(e)], gath.at[y, line // LINES, rows_of(line % LINES * NX + ex)],
                    send_sem, recv_sem.at[line // LINES], e, tp,
                )

    dispatch(packed, ty, disp_send, disp_recv)

    def exchange_down():
        for d in (2, 4, 6, 1, 3, 5, 7):
            t = (tp + d) % NT
            send(down_h.at[t % NC, :, quarter_of(t // NC)], wd.at[tp], wd_send, wd_recv, ep, t)

    send(gate_h.at[1 - tc], wall.at[0, tc], wall_send, wall_recv, ep, mate)
    send(up_h.at[1 - tc], wall.at[1, tc], wall_send, wall_recv, ep, mate)

    if WD_AT == 0:
        exchange_down()


    far = (ty + 2) % NY
    if FAR_AT == 0:
        pack(far, spare)
        dispatch(spare, far, far_send, far_recv, FAR_FAR)

    with jax.named_scope("p_combine"):
        number = lax.broadcasted_iota(jnp.int32, (NE * NC, rows), 0)
        every, weights = placed(number % NE * NC + number // NE)
        w_slots = jnp.where(every, weights[:, None, :], 0.0).reshape(NE * block, rows)
        for c in range(NC):
            combine[c] = w_slots[c * NE * cap : (c + 1) * NE * cap].T

    if WD_AT == 1:
        exchange_down()
    if FAR_AT == 2:
        pack(far, spare)
        dispatch(spare, far, far_send, far_recv, FAR_FAR)

    with jax.named_scope("p_columns"):
        load_gate.wait()
        load_up.wait()
        arrived(wall.at[0], wall_recv)
        for i in range(0, features, quarter):
            columns[i : i + quarter, :] = wall[:, :, :, i : i + quarter].reshape(2 * NC * half, quarter).T

    if FAR_AT == 1:
        pack(far, spare)
        dispatch(spare, far, far_send, far_recv, FAR_FAR)

    def share_out(buf, y, q, send_sem, recv_sem, to, part=None):
        ref = buf.at[y, q] if part is None else buf.at[y, q, part]
        send(ref, ref, send_sem, recv_sem, ep, to * NC + tc)

    def along(dy):
        return (ty + dy) % NY

    def from_sources(y, q, recv_sem):
        @pl.when(own_q == q)
        def _():
            arrived(gath.at[y, q, pl.ds(0, chunk_rows - block)], recv_sem.at[q])

        @pl.when(own_q != q)
        def _():
            arrived(gath.at[y, q], recv_sem.at[q])

    def stage_a(q):
        from_sources(ty, q, disp_recv)
        share_out(gath, ty, q, ag_send, ag_recv.at[ty, q], along(1))
        share_out(gath, ty, q, ag_send, ag_recv.at[ty, q], along(3))

    def stage_d(q):
        from_sources(far, q, far_recv)
        for dy in (1, 3):
            arrived(gath.at[along(dy), q], ag_recv.at[along(dy), q])
        parts = []
        for y in range(NY):
            both = gath[y, q].astype(F32).reshape(PER, NC, cap, share)
            parts += [both[:, i].reshape(work_rows, share).astype(BF16) for i in range(NC)]
        x = jnp.concatenate(parts, axis=-1)
        both = jnp.dot(x, columns[...], preferred_element_type=F32)
        g, u = both[:, : NC * half], both[:, NC * half :]
        hid[ty, q] = (g / (1.0 + jnp.exp(-g)) * u).astype(BF16)
        for dy in (2, 1, 3):
            share_out(hid, ty, q, hid_send, hid_recv.at[q], along(dy))

    def stage_f(q):
        if q == 0:
            load_down.wait()
            arrived(wd.at[pl.ds(0, NT - 1)], wd_recv)
        arrived(hid.at[pl.ds(0, NY - 1), q], hid_recv.at[q])
        x = jnp.concatenate([hid[y, q] for y in range(NY)], axis=-1)
        result = jnp.dot(x, wd[...].reshape(NT * half, quarter), preferred_element_type=F32)
        top = jnp.maximum(jnp.max(jnp.abs(result), axis=-1, keepdims=True), 1e-30)
        key = jnp.ceil(jnp.log2(top) * KEYS) + 1.0
        level = jnp.round(result * (LEVELS * jnp.exp2(key * (-1.0 / KEYS)))).astype(jnp.int32)
        for c in range(NC):
            left = level[:, c * share : c * share + 128]
            right = level[:, c * share + 128 : (c + 1) * share]
            outb[pl.ds(c * NE + q * PER, PER), 0:cap, :] = ((left << 16) | (right & 0xFFFF)).reshape(PER, cap, 128)
        row = lax.broadcasted_iota(jnp.int32, (work_rows, 128), 0) % cap
        col = lax.broadcasted_iota(jnp.int32, (work_rows, 128), 1)
        keys = jnp.where(col == row + ep % (128 // cap) * cap, key, 0.0)
        keys = jnp.sum(keys.reshape(PER, cap, 128), axis=1, keepdims=True).astype(jnp.int32)
        for c in range(NC):
            outb[pl.ds(c * NE + q * PER, PER), cap : cap + 1, :] = keys

        @pl.when(own_q == q)
        def _():
            r = own_line % LINES * NX + ex
            ret[tc, ep] = outb[tc * NE + q * PER + r]

        for k in range(LINES):
            line = q * LINES + k
            z = ZORDER[line] if ABSOLUTE else (ez + ORDER[line]) % NZ

            @pl.loop(0, NX)
            def _(x):
                e, r = z * NX + x, k * NX + x
                for c in range(NC):

                    @pl.when((e != ep) | (c != tc))
                    def _():
                        t = ty * NC + c
                        send(outb.at[c * NE + q * PER + r], ret.at[tc, ep], ret_send, ret_recv.at[tc], e, t)

    stages = {"a": stage_a, "d": stage_d, "f": stage_f}
    for word in SEQ:
        with jax.named_scope(f"stage_{word}"):
            stages[word[0]](int(word[1:]))

    per = 128 // cap
    total = jnp.zeros(out_v.shape, F32)
    for c in (1, 0):
        with jax.named_scope(f"ret_wait{c}"):

            @pl.when(tc == c)
            def _():
                arrived(ret.at[c, pl.ds(0, NE - 1)], ret_recv.at[c])

            @pl.when(tc != c)
            def _():
                arrived(ret.at[c], ret_recv.at[c])

        words = ret[c, :, 0:cap, :].reshape(NE * cap, 128)
        back = jnp.concatenate([words >> 16, (words << 16) >> 16], axis=-1)
        keys = ret[c, :, cap : cap + 1, :].astype(F32)
        keys = jnp.concatenate([jnp.sum(keys[i : i + per], axis=0) for i in range(0, NE, per)], axis=-1)
        scale = jnp.exp2(keys * (1.0 / KEYS)) * (1.0 / LEVELS)
        total = total + weighted(combine[c] * scale, back)
    out_v[...] = total.astype(out_v.dtype)

    with jax.named_scope("drain"):
        arrived(packed.at[pl.ds(0, (NE - 1) * block)], disp_send)
        arrived(wd.at[pl.ds(0, NT - 1)], wd_send)
        arrived(wall.at[0], wall_send)
        arrived(gath.at[pl.ds(0, 2)], ag_send)
        arrived(packed.at[pl.ds(0, (NE - 1) * block)], far_send)
        arrived(hid.at[pl.ds(0, NY - 1)], hid_send)
        arrived(outb.at[pl.ds(0, NE * NC - 1)], ret_send)


def per_device(tokens, norm_gain, norm_shift, expert_ids, gate_weights, expert_gate, expert_up, expert_down):
    rows, features = tokens.shape
    local, _, half = expert_gate.shape
    quarter = features // NY
    share = features // NT
    cap = rows // 2 * expert_ids.shape[1] // (local * NE // GROUPS)
    block = local * cap
    any_spec = pl.BlockSpec(memory_space=pl.ANY)
    vmem = pl.BlockSpec(memory_space=pltpu.VMEM)
    dma = pltpu.SemaphoreType.DMA
    out = pl.pallas_call(
        kernel,
        out_shape=pltpu.VMEM((rows, share), F32),
        in_specs=[any_spec, vmem, vmem, vmem, vmem, any_spec, any_spec, any_spec],
        out_specs=vmem,
        scratch_shapes=[
            pltpu.VMEM((rows, features), BF16),
            pltpu.VMEM((2, NC, half, features), BF16),
            pltpu.VMEM((features, 2 * NC * half), BF16),
            pltpu.VMEM((NE * block, share), BF16),
            pltpu.VMEM((NE * block, share), BF16),
            pltpu.VMEM((NY, CHUNKS, PER * block, share), BF16),
            pltpu.VMEM((NT, half, quarter), BF16),
            pltpu.VMEM((NY, CHUNKS, PER * cap, NC * half), BF16),
            pltpu.VMEM((NE * NC, cap + 1, 128), jnp.int32),
            pltpu.VMEM((NC, NE, cap + 1, 128), jnp.int32),
            pltpu.VMEM((NC, rows, NE * cap), F32),
            dma((4,)),
            dma,
            dma((CHUNKS,)),
            dma,
            dma((CHUNKS,)),
            dma,
            dma((NY, CHUNKS)),
            dma,
            dma,
            dma,
            dma,
            dma,
            dma((CHUNKS,)),
            dma,
            dma((NC,)),
        ],
        compiler_params=pltpu.CompilerParams(collective_id=0, has_side_effects=True, vmem_limit_bytes=VMEM_LIMIT),
    )(
        tokens,
        norm_gain.reshape(1, features),
        norm_shift.reshape(1, features),
        expert_ids.T,
        gate_weights.T,
        expert_gate.transpose(0, 2, 1),
        expert_up.transpose(0, 2, 1),
        expert_down,
    )
    return out.astype(BF16)


def solution(mesh):
    return jax.shard_map(
        per_device,
        mesh=mesh,
        in_specs=(
            P("ep", None),
            P(),
            P(),
            P("ep", None),
            P("ep", None),
            P("ep", None, "tp"),
            P("ep", None, "tp"),
            P("ep", "tp", None),
        ),
        out_specs=P("ep", "tp"),
        check_vma=False,
    )
```
